512 devices in a mesh: sp: 64 (over z, y), tp: 8 (over x, core).
Axes of the slice: x: 4, y: 8, z: 8, core: 2. Of those that a mesh axis runs over, the one named last changes fastest.
Arguments:
- skip_stream_entering: bfloat16 [4096, 2048], P('sp'), may hold values from -6 to 6
- reading_vectors: bfloat16 [4096, 1024], P('sp', 'tp'), may hold values from -6 to 6
- blender_lookup_labels: bfloat16 [4096, 1024], P('sp', 'tp'), may hold values from -6 to 6
- blender_payloads: bfloat16 [4096, 1024], P('sp', 'tp'), may hold values from -6 to 6
- blender_result_valve: bfloat16 [4096, 1024], P('sp', 'tp'), may hold values from -6 to 6
- fading_logits: bfloat16 [2, 4096, 1024], P(None, 'sp', 'tp'), as said below
- amend_speed_logits: bfloat16 [2, 4096, 1024], P(None, 'sp', 'tp'), as said below
- extra_log_fades: float32 [2, 16, 4096], P(None, 'tp', 'sp'), may hold values from -3 to 0
- present_reward_factors: float32 [1024], P('tp'), may hold values from -1.2 to 1.2
- attender_scaling_vector: float32 [1024], P('tp'), may hold values from 0.1 to 1.9
- blender_result_projector: bfloat16 [1024, 2048], P('tp'), may hold values from -0.1875 to 0.1875
- blender_scaling_vector: float32 [2048], replicated, may hold values from 0.1 to 1.9
- perceptron_valve_factors: bfloat16 [2048, 5632], P('sp', 'tp'), may hold values from -0.125 to 0.125
- perceptron_widen_factors: bfloat16 [2048, 5632], P('sp', 'tp'), may hold values from -0.125 to 0.125
- perceptron_shrink_factors: bfloat16 [5632, 2048], P('tp', 'sp'), may hold values from -0.078125 to 0.078125
- closing_scaling_vector: float32 [2048], replicated, may hold values from 0.1 to 1.9
Outputs:
- result: bfloat16 [4096, 2048], P(('sp', 'tp'))
The draws below stay inside these ranges and needn't reach their ends.
Inputs may be any that keep to these rules, and one draw needn't show every extreme that they name: `fading_logits`: decay pre-activations. `amend_speed_logits`: correction-rate pre-activations.
All inputs are finite; a program needn't handle non-finite values.
Results may differ from the reference program's by a relative error of at most 0.02.
Values may be sent and summed in bfloat16 or wider, within the bound.
A program may use at most 64 MiB of HBM per device.

```python
import math
import jax
import jax.numpy as jnp
from jax import lax

D = 2048
FF = 5632
HEADS = 16
HEAD = 64
TOK_DEV = 64
STRING_LENGTH = 4096
BLENDER_WIDTH = 1024
N_TP = 8


def head_classes(key):
    picked = jax.random.uniform(jax.random.fold_in(key, 101), (2, HEADS), jnp.float32)
    slow_share = 0.5
    mixed_index = jax.random.randint(jax.random.fold_in(key, 102), (2,), 0, HEADS)
    mixed = (jnp.arange(HEADS, dtype=jnp.int32)[None, :] == mixed_index[:, None]).astype(jnp.float32)
    slow = (picked < slow_share).astype(jnp.float32) * (1.0 - mixed)
    return (slow, mixed)


def fast_blocks(key):
    block_count = STRING_LENGTH // TOK_DEV
    phase = jax.random.randint(jax.random.fold_in(key, 103), (2,), 0, 8)
    place = (jnp.arange(block_count, dtype=jnp.int32)[None, :] + phase[:, None]) % 8
    extra = jax.random.randint(jax.random.fold_in(key, 104), (2, block_count), 0, 2)
    return jnp.where(place == 4, 1.0, jnp.where(place == 0, extra.astype(jnp.float32), 0.0))


def draw_fading_logits(key, part):
    slow, mixed = head_classes(key)
    block_count = STRING_LENGTH // TOK_DEV
    quick = fast_blocks(key)
    slow_now = slow[:, None, :] + mixed[:, None, :] * (1.0 - quick[:, :, None])
    slow_now = jnp.broadcast_to(slow_now[:, :, None, :], (2, block_count, TOK_DEV, HEADS)).reshape(2, STRING_LENGTH, HEADS)
    slow_cols = jnp.repeat(slow_now, HEAD, axis=2)
    base_vals = slow_cols * (-math.log(STRING_LENGTH) - 0.2) + (1.0 - slow_cols) * -4.0
    offsets = jax.random.uniform(jax.random.fold_in(key, 11), (2, block_count, 1, HEADS), jnp.float32, -0.7, 0.7)
    offsets = jnp.broadcast_to(offsets, (2, block_count, TOK_DEV, HEADS)).reshape(2, STRING_LENGTH, HEADS)
    offsets = jnp.repeat(offsets, HEAD, axis=2)
    noise_vals = jnp.clip(0.5 * jax.random.normal(jax.random.fold_in(key, 12), (2, STRING_LENGTH, BLENDER_WIDTH), jnp.float32), -1.5, 1.5)
    return (base_vals + offsets + noise_vals).astype(jnp.bfloat16)


def draw_amend_speed_logits(key, part):
    slow, mixed = head_classes(key)
    slow_cols = jnp.repeat(slow + mixed, HEAD, axis=1)
    base_vals = slow_cols * math.log(32.0 / STRING_LENGTH)
    noise_vals = jnp.clip(0.7 * jax.random.normal(jax.random.fold_in(key, 21), (2, STRING_LENGTH, BLENDER_WIDTH), jnp.float32), -2.0, 2.0)
    return (base_vals[:, None, :] + noise_vals).astype(jnp.bfloat16)


def draw_extra_log_fades(key, part):
    spots = jax.random.randint(jax.random.fold_in(key, 31), (2, HEADS, 6), 0, STRING_LENGTH)
    depths = jnp.log(jax.random.uniform(jax.random.fold_in(key, 32), (2, HEADS, 6), jnp.float32, 0.5, 0.8))
    places = jnp.arange(STRING_LENGTH, dtype=jnp.int32)
    hits = (spots[..., None] == places).astype(jnp.float32)
    return jnp.einsum('dhb,dhbt->dht', depths, hits)


def levels(stream_key, dims, pieces, least, top_value):
    def one(dim, shards_of):
        draws = jax.random.uniform(jax.random.fold_in(jax.random.fold_in(stream_key, 6), dim), (shards_of,), jnp.float32, least / len(pieces), top_value / len(pieces))
        return jnp.repeat(jnp.exp(draws), dims[dim] // shards_of).reshape((-1,) + (1,) * (len(dims) - dim - 1))

    factor_of = one(*pieces[0])
    for cut in pieces[1:]:
        factor_of = factor_of * one(*cut)
    return factor_of


def scatter_about(key, dims, scale, most, split=(), kind=jnp.bfloat16):
    level = levels(key, dims, split, -0.22, 0.18) if split else 1.0
    values = jax.random.normal(key, dims, jnp.float32) * scale * level
    return jnp.minimum(jnp.maximum(values, -most), most).astype(kind)


def setup_inputs(seed: int = 0) -> dict:
    key_list = jax.random.split(jax.random.key(seed), 17)
    return {
        "skip_stream_entering": scatter_about(key_list[0], (STRING_LENGTH, D), 1.0, 6.0, ((0, 64),)),
        "reading_vectors": scatter_about(key_list[1], (STRING_LENGTH, BLENDER_WIDTH), 1.0, 6.0, ((0, 64), (1, 8))),
        "blender_lookup_labels": scatter_about(key_list[2], (STRING_LENGTH, BLENDER_WIDTH), 1.0, 6.0, ((0, 64), (1, 8))),
        "blender_payloads": scatter_about(key_list[3], (STRING_LENGTH, BLENDER_WIDTH), 1.0, 6.0, ((0, 64), (1, 8))),
        "blender_result_valve": scatter_about(key_list[4], (STRING_LENGTH, BLENDER_WIDTH), 1.0, 6.0, ((0, 64), (1, 8))),
        "fading_logits": draw_fading_logits(jax.random.fold_in(key_list[16], 71), 0),
        "amend_speed_logits": draw_amend_speed_logits(jax.random.fold_in(key_list[16], 71), 0),
        "extra_log_fades": draw_extra_log_fades(jax.random.fold_in(key_list[16], 71), 0),
        "present_reward_factors": scatter_about(key_list[8], (BLENDER_WIDTH,), 0.2, 1.2, ((0, 8),), jnp.float32),
        "attender_scaling_vector": jnp.clip(1.0 + 0.18 * jax.random.normal(key_list[9], (BLENDER_WIDTH,), jnp.float32), 0.1, 1.9),
        "blender_result_projector": scatter_about(key_list[10], (BLENDER_WIDTH, D), BLENDER_WIDTH ** -0.5, 0.1875, ((0, 8),)),
        "blender_scaling_vector": jnp.clip(1.0 + 0.18 * jax.random.normal(key_list[11], (D,), jnp.float32), 0.1, 1.9),
        "perceptron_valve_factors": scatter_about(key_list[12], (D, FF), D ** -0.5, 0.125, ((0, 64), (1, 8))),
        "perceptron_widen_factors": scatter_about(key_list[13], (D, FF), D ** -0.5, 0.125, ((0, 64), (1, 8))),
        "perceptron_shrink_factors": scatter_about(key_list[14], (FF, D), FF ** -0.5, 0.078125, ((0, 8), (1, 64))),
        "closing_scaling_vector": jnp.clip(1.0 + 0.18 * jax.random.normal(key_list[15], (D,), jnp.float32), 0.1, 1.9),
    }


RESIDUAL_SCALE = 2.0 ** 0.25
NORM_EPS = 1e-05
GROUP_EPS = 0.00064
KEY_EPS = 1e-06
PRECISE = lax.Precision.HIGHEST

def layer_norm(summand, gain_vec):
    center = lax.optimization_barrier(jnp.mean(summand, -1, keepdims=True))
    spread = lax.optimization_barrier(jnp.mean(jnp.square(summand - center), -1, keepdims=True))
    return (summand - center) * lax.rsqrt(spread + NORM_EPS) * gain_vec

def wire_round(tensor):
    return lax.optimization_barrier(tensor.astype(jnp.bfloat16)).astype(jnp.float32)

def direction_scan(entire_asking_lines, decays, stored_label_lines, payload_line_slab, erase_keys, refills):

    def advance(state_mat, inputs):
        query_vec, decay_vec, write_key, value_vec, erase_vec, refill_vec = inputs
        erased = jnp.einsum('hij,hj->hi', state_mat, erase_vec, precision=PRECISE)
        state_mat = state_mat * decay_vec[:, None, :] + erased[:, :, None] * refill_vec[:, None, :] + value_vec[:, :, None] * write_key[:, None, :]
        return (state_mat, jnp.einsum('hij,hj->hi', state_mat, query_vec, precision=PRECISE))
    start_state = jnp.zeros((HEADS, HEAD, HEAD), jnp.float32)
    _, outputs = lax.scan(advance, start_state, (entire_asking_lines, decays, stored_label_lines, payload_line_slab, erase_keys, refills))
    return outputs

def reference(skip_stream_entering, reading_vectors, blender_lookup_labels, blender_payloads, blender_result_valve, fading_logits, amend_speed_logits, extra_log_fades, present_reward_factors, attender_scaling_vector, blender_result_projector, blender_scaling_vector, perceptron_valve_factors, perceptron_widen_factors, perceptron_shrink_factors, closing_scaling_vector):

    def split_attenders(tensor):
        return tensor.reshape(tensor.shape[:-1] + (HEADS, HEAD))

    def flipped(tensor):
        return jnp.flip(tensor, 0)
    entire_asking_lines = split_attenders(reading_vectors.astype(jnp.float32))
    key_rows = split_attenders(blender_lookup_labels.astype(jnp.float32))
    payload_line_slab = split_attenders(blender_payloads.astype(jnp.float32))
    key_square = lax.optimization_barrier(jnp.sum(key_rows * key_rows, -1, keepdims=True))
    unit_keys = key_rows * lax.rsqrt(key_square + KEY_EPS)
    fading_log_amount = split_attenders(-jnp.exp(-jax.nn.softplus(-fading_logits.astype(jnp.float32)) - 0.5)) + jnp.swapaxes(extra_log_fades, 1, 2)[..., None]
    decays = jnp.exp(fading_log_amount)
    icl_rates = split_attenders(jax.nn.sigmoid(amend_speed_logits.astype(jnp.float32)))
    stored_label_lines = key_rows[None] * icl_rates
    refills = unit_keys[None] * icl_rates
    forward = direction_scan(entire_asking_lines, decays[0], stored_label_lines[0], payload_line_slab, -unit_keys, refills[0])
    backward = flipped(direction_scan(flipped(entire_asking_lines), flipped(decays[1]), flipped(stored_label_lines[1]), flipped(payload_line_slab), flipped(-unit_keys), flipped(refills[1])))
    summed = forward + backward
    center = lax.optimization_barrier(jnp.mean(summed, -1, keepdims=True))
    spread = lax.optimization_barrier(jnp.mean(jnp.square(summed - center), -1, keepdims=True))
    rescaled_lines = (summed - center) * lax.rsqrt(spread + GROUP_EPS) * split_attenders(attender_scaling_vector)
    present_reward_summand = lax.optimization_barrier(jnp.sum(entire_asking_lines * (stored_label_lines[0] + stored_label_lines[1]) * split_attenders(present_reward_factors), -1, keepdims=True)) * payload_line_slab
    merged_attender_lines = ((rescaled_lines + present_reward_summand) * split_attenders(blender_result_valve.astype(jnp.float32))).reshape(STRING_LENGTH, BLENDER_WIDTH)
    merged_attender_lines = merged_attender_lines.astype(jnp.bfloat16)
    group_cols = BLENDER_WIDTH // N_TP
    mixsum = jnp.zeros((STRING_LENGTH, D), jnp.float32)
    for index in range(N_TP):
        partial_mix = jnp.dot(merged_attender_lines[:, index * group_cols:(index + 1) * group_cols], blender_result_projector[index * group_cols:(index + 1) * group_cols], preferred_element_type=jnp.float32)
        mixsum = mixsum + wire_round(partial_mix)
    middle = layer_norm(RESIDUAL_SCALE * skip_stream_entering.astype(jnp.float32) + mixsum, blender_scaling_vector).astype(jnp.bfloat16)
    group_units = FF // N_TP

    def ffn_block(block_rows):
        gate_pre = jnp.dot(block_rows, perceptron_valve_factors, preferred_element_type=jnp.float32)
        up_pre = jnp.dot(block_rows, perceptron_widen_factors, preferred_element_type=jnp.float32)
        inner_act = (jax.nn.silu(gate_pre) * up_pre).astype(jnp.bfloat16)
        downsum = jnp.zeros((block_rows.shape[0], D), jnp.float32)
        for index in range(N_TP):
            partial_down = jnp.dot(inner_act[:, index * group_units:(index + 1) * group_units], perceptron_shrink_factors[index * group_units:(index + 1) * group_units], preferred_element_type=jnp.float32)
            downsum = downsum + wire_round(partial_down)
        return layer_norm(RESIDUAL_SCALE * block_rows.astype(jnp.float32) + downsum, closing_scaling_vector).astype(jnp.bfloat16)
    blocked = lax.map(ffn_block, middle.reshape(STRING_LENGTH // TOK_DEV, TOK_DEV, D))
    return blocked.reshape(STRING_LENGTH, D)
```

```python
import jax
import jax.numpy as jnp
from jax import lax
from jax.experimental import pallas as pl
from jax.experimental.pallas import tpu as pltpu
from jax.sharding import Mesh
from jax.sharding import PartitionSpec as P

SP = ("sp_0", "sp_1")
SP_TP = ("sp_0", "sp_1", "tp")
MESH = pl.DeviceIdType.MESH
F32 = jnp.float32
BF16 = jnp.bfloat16
HIGHEST = lax.Precision.HIGHEST

RESIDUAL_SCALE = 2.0**0.25
NORM_EPS = 1e-05
GROUP_EPS = 0.00064
KEY_EPS = 1e-06
HALF_EXP = 0.6065306597126334

TOK = 64
LANES = 128
WA_COLS = 1152
WB_COLS = 1024


def dot(a, b, ca=1, cb=0):
    return lax.dot_general(
        a, b, (((ca,), (cb,)), ((), ())), precision=HIGHEST, preferred_element_type=F32
    )


def bdot(a, b, ca=1, cb=0):
    return lax.dot_general(
        a.astype(BF16), b.astype(BF16), (((ca,), (cb,)), ((), ())), preferred_element_type=F32
    )


def iota(shape, dim):
    return lax.broadcasted_iota(jnp.int32, shape, dim)


def expand(x):
    lane = iota(x.shape, 1)
    zero = jnp.zeros_like(x)
    return jnp.concatenate([jnp.where(lane < 64, x, zero), jnp.where(lane >= 64, x, zero)], 0)


def fold(z):
    half = z.shape[0] // 2
    return z[:half] + z[half:]


def head_ones():
    return jnp.where((iota((128, 128), 0) < 64) == (iota((128, 128), 1) < 64), 1.0, 0.0).astype(F32)


def local_mixer(q, key, val, inv, fade, amend, extra, d):
    row, col = iota((64, 64), 0), iota((64, 64), 1)
    k = key * jax.nn.sigmoid(amend)
    logw = extra - jax.nn.sigmoid(fade) * HALF_EXP
    tri = jnp.where(col <= row if d == 0 else col >= row, 1.0, 0.0).astype(F32)
    c = dot(tri, logw)
    cx = c - logw
    end = c[63:64] if d == 0 else c[0:1]
    un = key * inv * inv
    erase_rows, read_rows = [], []
    for i in range(4):
        lo = 16 * i
        ref = cx[lo : lo + 1] if d == 0 else cx[lo + 15 : lo + 16]
        kk = k * jnp.exp(jnp.minimum(ref - c, 60.0))
        lu = un[lo : lo + 16] * jnp.exp(cx[lo : lo + 16] - ref)
        lq = q[lo : lo + 16] * jnp.exp(c[lo : lo + 16] - ref)
        res = bdot(jnp.concatenate([lu, lq], 0), expand(kk), 1, 1)
        erase_rows.append(res[:16])
        read_rows.append(res[16:])
    m_all = jnp.concatenate(erase_rows, 0)
    g_all = jnp.concatenate(read_rows, 0)
    rt, ct = iota((64, 128), 0), iota((64, 128), 1) & 63
    m_all = expand(jnp.where(ct < rt if d == 0 else ct > rt, m_all, 0.0))
    g_all = jnp.where(ct <= rt if d == 0 else ct >= rt, g_all, 0.0)
    r, cc = iota((128, 128), 0), iota((128, 128), 1)
    eye = jnp.where(r == cc, 1.0, 0.0).astype(F32)
    inverse = eye - jnp.where((r >> 1) == (cc >> 1), m_all, 0.0)
    for b in range(1, 6):
        off = jnp.where(((r >> (b + 1)) == (cc >> (b + 1))) & ((r >> b) != (cc >> b)), m_all, 0.0)
        inverse = inverse - dot(dot(inverse, off), inverse)
    ut = un * jnp.exp(cx)
    vw = dot(inverse, jnp.concatenate([expand(val), expand(ut)], 1))
    kend = expand(k * jnp.exp(end - c))
    z = bdot(vw, kend, 0, 0)
    written = fold(z[:128])
    passed = jnp.where(rt == ct, jnp.exp(end), 0.0) - fold(z[128:])
    return k, passed, written, g_all, vw, q * jnp.exp(c)


def body(
    skip_ref, q_ref, key_ref, val_ref, valve_ref, fade_ref, amend_ref, extra_ref, bonus_ref,
    again_ref, proj_ref, mgain_ref, wa_ref, wb_ref, cgain_ref, out_ref,
    wa, wb, pb, c1s, c1r, c2s, c2r, c3s, c3r, mb, rs, rr, midf, midb, gu,
    a1s, a1r, b1s, b1r, a2s, a2r, b2s, b2r, p1s, p1r, p2s, p2r, p3s, p3r,
    x1s, x1r, x2s, x2r, x3s, x3r, ms, mr, ds, dr,
):
    z, y, tp = lax.axis_index("sp_0"), lax.axis_index("sp_1"), lax.axis_index("tp")
    xc, core = tp // 2, tp % 2
    partner = tp + 1 - 2 * core

    def up(at, j, n=8):
        return lax.rem(at + j, n)

    def down(at, j, n=8):
        return lax.rem(at + n - j, n)

    def copy(src, dst, send, recv, axis, at):
        return pltpu.make_async_remote_copy(
            src_ref=src, dst_ref=dst, send_sem=send, recv_sem=recv,
            device_id={axis: at}, device_id_type=MESH,
        )

    barrier = pltpu.get_barrier_semaphore()
    for axis, at in (("sp_0", z), ("sp_1", y), ("tp", tp)):
        for j in range(1, 8):
            pl.semaphore_signal(barrier, inc=1, device_id={axis: up(at, j)}, device_id_type=MESH)
    pl.semaphore_wait(barrier, 21)

    sent = []

    def go(c):
        c.start()
        sent.append(c)

    order = (1, 7, 2, 6, 3, 5, 4)
    for j in order:
        go(copy(wa_ref, wa.at[z, y], a1s.at[j - 1], a1r.at[j - 1], "sp_1", up(y, j)))
        go(copy(wb_ref, wb.at[z, y], b1s.at[j - 1], b1r.at[j - 1], "sp_0", up(z, j)))
    for j in (1, 3, 2):
        go(copy(proj_ref, pb.at[tp], p1s.at[j - 1], p1r.at[j - 1], "tp", 2 * up(xc, j, 4) + core))
    go(copy(proj_ref, pb.at[tp], p2s.at[0], p2r.at[0], "tp", partner))
    wa[z, y] = wa_ref[...]
    wb[z, y] = wb_ref[...]
    pb[tp] = proj_ref[...]

    q, key, val = q_ref[...].astype(F32), key_ref[...].astype(F32), val_ref[...].astype(F32)
    ones = head_ones()
    inv = lax.rsqrt(dot(key * key, ones) + KEY_EPS)
    sides = []
    for d in range(2):
        k, passed, written, g_all, vw, qc = local_mixer(
            q, key, val, inv, fade_ref[d].astype(F32), amend_ref[d].astype(F32), extra_ref[d], d
        )
        passed, written = passed.astype(BF16), written.astype(BF16)
        for part in range(4):
            c1s[4 * d + part] = jnp.concatenate([passed, written[16 * part : 16 * part + 16]], 0)
        sides.append((k, g_all, vw, qc))
    for j in order:
        w = up(y, j)
        go(copy(c1s.at[w], c1r.at[y], x1s.at[j - 1], x1r.at[j - 1], "sp_1", w))
    c1r[y] = c1s[y]

    reads = []
    for k, g_all, vw, qc in sides:
        oy = bdot(g_all, vw)
        reads.append((oy[:, :128], (qc - oy[:, 128:]).astype(BF16)))
    bonus = dot(q * (sides[0][0] + sides[1][0]) * bonus_ref[...], ones) * val

    for j in order:
        copy(c1s.at[y], c1r.at[down(y, j)], x1s.at[j - 1], x1r.at[j - 1], "sp_1", y).wait_recv()
    side = y // 4
    both = jnp.where(iota((64, 128), 0) == (iota((64, 128), 1) & 63), 1.0, 0.0).astype(F32)
    joined = jnp.concatenate([both, jnp.zeros((16, 128), F32)], 0)
    fresh = jnp.zeros((64, 128), F32)
    prefixes = []
    for n in range(8):
        prefixes.append(joined)
        block = c1r[n + side * (7 - 2 * n)]
        joined = bdot(joined, expand(block[:64])) + jnp.concatenate(
            [fresh, block[64:].astype(F32)], 0
        )
    c2s[...] = joined.astype(BF16)
    c2r[z] = joined.astype(BF16)
    for j in order:
        go(copy(c2s, c2r.at[z], x2s.at[j - 1], x2r.at[j - 1], "sp_0", up(z, j)))

    def ring(s, start):
        last = s == 4
        first, second = (slice(0, 4), slice(4, 8)) if last else (slice(0, 8), slice(0, 8))
        n = down(z, s - 1) if start else down(z, s)
        m = up(z, s - 1) if start else up(z, s)
        u = down(y, s - 1) if start else down(y, s)
        v = up(y, s - 1) if start else up(y, s)
        four = (
            copy(wa.at[n, first], wa.at[n, first], a2s.at[0, s - 1], a2r.at[0, s - 1], "sp_0", up(z, 1)),
            copy(wa.at[m, second], wa.at[m, second], a2s.at[1, s - 1], a2r.at[1, s - 1], "sp_0", down(z, 1)),
            copy(wb.at[first, u], wb.at[first, u], b2s.at[0, s - 1], b2r.at[0, s - 1], "sp_1", up(y, 1)),
            copy(wb.at[second, v], wb.at[second, v], b2s.at[1, s - 1], b2r.at[1, s - 1], "sp_1", down(y, 1)),
        )
        for c in four:
            if start:
                go(c)
            else:
                c.wait_recv()

    for j in order:
        copy(wa_ref, wa.at[z, down(y, j)], a1s.at[j - 1], a1r.at[j - 1], "sp_1", y).wait_recv()
        copy(wb_ref, wb.at[down(z, j), y], b1s.at[j - 1], b1r.at[j - 1], "sp_0", z).wait_recv()
    ring(1, True)

    for j in order:
        copy(c2s, c2r.at[down(z, j)], x2s.at[j - 1], x2r.at[j - 1], "sp_0", z).wait_recv()
    entering = jnp.zeros((16, 128), F32)
    for n in range(8):
        at = n + side * (7 - 2 * n)
        block = c2r[at]
        new = bdot(entering, expand(block[:64])) + block[64:].astype(F32)
        before = (1 - 2 * side) * (z - at) > 0
        entering = jnp.where(before, new, entering)
    for n in range(8):
        before = prefixes[n]
        c3s[n + side * (7 - 2 * n)] = (
            bdot(entering, expand(before[:64])) + before[64:]
        ).astype(BF16)
    for j in order:
        w = up(y, j)
        go(copy(c3s.at[w], c3r.at[y], x3s.at[j - 1], x3r.at[j - 1], "sp_1", w))
    c3r[y] = c3s[y]

    for j in (1, 3, 2):
        at = 2 * down(xc, j, 4) + core
        copy(proj_ref, pb.at[at], p1s.at[j - 1], p1r.at[j - 1], "tp", tp).wait_recv()
        go(copy(pb.at[at], pb.at[at], p3s.at[j - 1], p3r.at[j - 1], "tp", partner))

    ring(1, False)
    ring(2, True)

    for j in order:
        copy(c3s.at[y], c3r.at[down(y, j)], x3s.at[j - 1], x3r.at[j - 1], "sp_1", y).wait_recv()
    summed = jnp.zeros((64, 128), F32)
    for d in range(2):
        state = jnp.concatenate([c3r[4 * d + part] for part in range(4)], 0)
        summed = summed + reads[d][0] + bdot(reads[d][1], expand(state), 1, 1)
    center = dot(summed, ones) * (1.0 / 64)
    away = summed - center
    spread = dot(away * away, ones) * (1.0 / 64)
    normed = away * lax.rsqrt(spread + GROUP_EPS) * again_ref[...]
    mixed = (normed + bonus) * valve_ref[...].astype(F32)
    mb[tp] = mixed.astype(BF16)
    for j in order:
        go(copy(mb.at[tp], mb.at[tp], ms.at[j - 1], mr.at[j - 1], "tp", up(tp, j)))
    copy(proj_ref, pb.at[partner], p2s.at[0], p2r.at[0], "tp", tp).wait_recv()
    for j in (1, 3, 2):
        at = 2 * down(xc, j, 4) + 1 - core
        copy(pb.at[at], pb.at[at], p3s.at[j - 1], p3r.at[j - 1], "tp", tp).wait_recv()
    for j in order:
        copy(mb.at[tp], mb.at[down(tp, j)], ms.at[j - 1], mr.at[j - 1], "tp", tp).wait_recv()

    rows = jnp.concatenate([mb[n] for n in range(8)], 1)

    def project(n, carry):
        cols = pl.ds(pl.multiple_of(n * 256, 256), 256)
        weights = pb[:, :, cols].reshape(1024, 256)
        midf[:, cols] = RESIDUAL_SCALE * skip_ref[:, cols].astype(F32) + bdot(rows, weights)
        return carry

    lax.fori_loop(0, 8, project, 0)

    def layer_norm(x, gain):
        center = jnp.mean(x, -1, keepdims=True)
        away = x - center
        spread = jnp.mean(away * away, -1, keepdims=True)
        return away * lax.rsqrt(spread + NORM_EPS) * gain

    for n in range(8):
        part = slice(8 * n, 8 * n + 8)
        normal = layer_norm(midf[part, :], mgain_ref[...]).astype(BF16)
        midf[part, :] = normal.astype(F32)
    midb[...] = midf[...].astype(BF16)

    ring(2, False)
    ring(3, True)
    ring(3, False)
    ring(4, True)
    ring(4, False)

    gu[...] = jnp.zeros_like(gu)

    def widen(n, carry):
        mid = midb[:, pl.ds(pl.multiple_of(n * 256, 256), 256)]
        gu[:, :1152] += bdot(mid, wa[n].reshape(256, 1152))
        gu[:, 1152:] += bdot(mid, wb[n, :, :, :256].reshape(256, 256))
        return carry

    lax.fori_loop(0, 8, widen, 0)

    gate, wide = gu[:, :640], gu[:, 640:1280]
    tail = gu[:, 1280:]
    main = gate / (1.0 + jnp.exp(-gate)) * wide
    rest = tail / (1.0 + jnp.exp(-tail)) * pltpu.roll(tail, 64, 1)
    rest = jnp.where(iota((64, 128), 1) < 64, rest, 0.0)
    inner = jnp.concatenate([main, rest], 1).astype(BF16)

    def shrink(n, carry):
        cols = pl.ds(pl.multiple_of(n * 256, 256), 256)
        share = bdot(inner, wb[n, :, :, 256:].reshape(256, 768), 1, 1)
        for m in range(8):
            rs[m, :, cols] = share[8 * m : 8 * m + 8].astype(BF16)
        return carry

    lax.fori_loop(0, 8, shrink, 0)
    for j in order:
        go(copy(rs.at[up(tp, j)], rr.at[tp], ds.at[j - 1], dr.at[j - 1], "tp", up(tp, j)))
    rr[tp] = rs[tp]
    for j in order:
        copy(rs.at[tp], rr.at[down(tp, j)], ds.at[j - 1], dr.at[j - 1], "tp", tp).wait_recv()
    total = RESIDUAL_SCALE * midf[pl.ds(pl.multiple_of(tp * 8, 8), 8), :]
    for n in range(8):
        total = total + rr[n].astype(F32)
    out_ref[...] = layer_norm(total, cgain_ref[...]).astype(BF16)
    for c in sent:
        c.wait_send()


def shards(
    skip, reading, labels, payloads, valve, fading, amend, extra, bonus, again, projector,
    mgain, gate, wide, shrink, cgain,
):
    down_rows = jnp.swapaxes(shrink, 0, 1)
    wa = jnp.concatenate([gate[:, :640], wide[:, :512]], 1)
    wb = jnp.concatenate(
        [wide[:, 512:640], gate[:, 640:], wide[:, 640:], down_rows, jnp.zeros((32, 64), BF16)], 1
    )
    fades = jnp.repeat(jnp.swapaxes(extra, 1, 2), 64, axis=2)
    dma = pltpu.SemaphoreType.DMA
    sems = [(7,)] * 4 + [(2, 4)] * 4 + [(3,), (3,), (1,), (1,), (3,), (3,)] + [(7,)] * 10
    return pl.pallas_call(
        body,
        out_shape=jax.ShapeDtypeStruct((8, 2048), BF16),
        in_specs=[pl.BlockSpec(memory_space=pltpu.VMEM)] * 15,
        out_specs=pl.BlockSpec(memory_space=pltpu.VMEM),
        scratch_shapes=[
            pltpu.VMEM((8, 8, 32, WA_COLS), BF16),
            pltpu.VMEM((8, 8, 32, WB_COLS), BF16),
            pltpu.VMEM((8, 128, 2048), BF16),
            pltpu.VMEM((8, 80, 128), BF16),
            pltpu.VMEM((8, 80, 128), BF16),
            pltpu.VMEM((80, 128), BF16),
            pltpu.VMEM((8, 80, 128), BF16),
            pltpu.VMEM((8, 16, 128), BF16),
            pltpu.VMEM((8, 16, 128), BF16),
            pltpu.VMEM((8, 64, 128), BF16),
            pltpu.VMEM((8, 8, 2048), BF16),
            pltpu.VMEM((8, 8, 2048), BF16),
            pltpu.VMEM((64, 2048), F32),
            pltpu.VMEM((64, 2048), BF16),
            pltpu.VMEM((64, 1408), F32),
        ]
        + [dma(s) for s in sems],
        compiler_params=pltpu.CompilerParams(
            collective_id=0, has_side_effects=True, vmem_limit_bytes=48 * 1024 * 1024
        ),
    )(
        skip, reading, labels, payloads, valve, fading, amend, fades, bonus.reshape(1, 128),
        again.reshape(1, 128), projector, mgain.reshape(1, 2048), wa, wb, cgain.reshape(1, 2048),
    )


def solution(mesh):
    finer = Mesh(mesh.devices.reshape(8, 8, mesh.shape["tp"]), ("sp_0", "sp_1", "tp"))
    placed = (
        P(SP, None),
        P(SP, "tp"),
        P(SP, "tp"),
        P(SP, "tp"),
        P(SP, "tp"),
        P(None, SP, "tp"),
        P(None, SP, "tp"),
        P(None, "tp", SP),
        P("tp"),
        P("tp"),
        P("tp", None),
        P(),
        P(SP, "tp"),
        P(SP, "tp"),
        P("tp", SP),
        P(),
    )
    return jax.shard_map(
        shards, mesh=finer, in_specs=placed, out_specs=P(SP_TP, None), check_vma=False
    )
```

```python
import jax
import jax.numpy as jnp
from jax import lax
from jax.experimental import pallas as pl
from jax.experimental.pallas import tpu as pltpu
from jax.sharding import Mesh
from jax.sharding import PartitionSpec as P

SP = ("sp_0", "sp_1")
SP_TP = ("sp_0", "sp_1", "tp")
MESH = pl.DeviceIdType.MESH
F32 = jnp.float32
BF16 = jnp.bfloat16
HIGHEST = lax.Precision.HIGHEST

RESIDUAL_SCALE = 2.0**0.25
NORM_EPS = 1e-05
GROUP_EPS = 0.00064
KEY_EPS = 1e-06
HALF_EXP = 0.6065306597126334

TOK = 64
LANES = 128
WA_COLS = 1152
WB_COLS = 1024
PIECES = ((0, 1, 7, 2), (6, 3, 5, 4))


def dot(a, b, ca=1, cb=0):
    return lax.dot_general(
        a, b, (((ca,), (cb,)), ((), ())), precision=HIGHEST, preferred_element_type=F32
    )


def bdot(a, b, ca=1, cb=0):
    return lax.dot_general(
        a.astype(BF16), b.astype(BF16), (((ca,), (cb,)), ((), ())), preferred_element_type=F32
    )


def iota(shape, dim):
    return lax.broadcasted_iota(jnp.int32, shape, dim)


def expand(x):
    lane = iota(x.shape, 1)
    zero = jnp.zeros_like(x)
    return jnp.concatenate([jnp.where(lane < 64, x, zero), jnp.where(lane >= 64, x, zero)], 0)


def fold(z):
    half = z.shape[0] // 2
    return z[:half] + z[half:]


def head_ones():
    return jnp.where((iota((128, 128), 0) < 64) == (iota((128, 128), 1) < 64), 1.0, 0.0).astype(F32)


def local_mixer(q, key, val, inv, fade, amend, extra, d):
    row, col = iota((64, 64), 0), iota((64, 64), 1)
    k = key * jax.nn.sigmoid(amend)
    logw = extra - jax.nn.sigmoid(fade) * HALF_EXP
    tri = jnp.where(col <= row if d == 0 else col >= row, 1.0, 0.0).astype(F32)
    c = dot(tri, logw)
    cx = c - logw
    end = c[63:64] if d == 0 else c[0:1]
    un = key * inv * inv
    erase_rows, read_rows = [], []
    for i in range(4):
        lo = 16 * i
        ref = cx[lo : lo + 1] if d == 0 else cx[lo + 15 : lo + 16]
        kk = k * jnp.exp(jnp.minimum(ref - c, 60.0))
        lu = un[lo : lo + 16] * jnp.exp(cx[lo : lo + 16] - ref)
        lq = q[lo : lo + 16] * jnp.exp(c[lo : lo + 16] - ref)
        res = bdot(jnp.concatenate([lu, lq], 0), expand(kk), 1, 1)
        erase_rows.append(res[:16])
        read_rows.append(res[16:])
    m_all = jnp.concatenate(erase_rows, 0)
    g_all = jnp.concatenate(read_rows, 0)
    rt, ct = iota((64, 128), 0), iota((64, 128), 1) & 63
    m_all = expand(jnp.where(ct < rt if d == 0 else ct > rt, m_all, 0.0))
    g_all = jnp.where(ct <= rt if d == 0 else ct >= rt, g_all, 0.0)
    r, cc = iota((128, 128), 0), iota((128, 128), 1)
    eye = jnp.where(r == cc, 1.0, 0.0).astype(F32)
    inverse = eye - jnp.where((r >> 1) == (cc >> 1), m_all, 0.0)
    for b in range(1, 6):
        off = jnp.where(((r >> (b + 1)) == (cc >> (b + 1))) & ((r >> b) != (cc >> b)), m_all, 0.0)
        inverse = inverse - dot(dot(inverse, off), inverse)
    ut = un * jnp.exp(cx)
    vw = dot(inverse, jnp.concatenate([expand(val), expand(ut)], 1))
    kend = expand(k * jnp.exp(end - c))
    z = bdot(vw, kend, 0, 0)
    written = fold(z[:128])
    passed = jnp.where(rt == ct, jnp.exp(end), 0.0) - fold(z[128:])
    return k, passed, written, g_all, vw, q * jnp.exp(c)


def body(
    skip_hbm, q_hbm, key_hbm, val_hbm, valve_hbm, fade_hbm, amend_hbm, extra_hbm, bonus_hbm,
    again_hbm, proj_hbm, mgain_hbm, gate_hbm, wide_hbm, drow_hbm, cgain_hbm, out_ref,
    skip_ref, q_ref, key_ref, val_ref, valve_ref, fade_ref, amend_ref, extra_ref, bonus_ref,
    again_ref, mgain_ref, gate_ref, wide_ref, drow_ref, cgain_ref,
    wa, wb, pb, c1s, c1r, c2s, c2r, c3s, c3r, mb, rs, rr, midf, midb, gu,
    a1s, a1r, b1s, b1r, a2s, a2r, b2s, b2r, p1s, p1r, p2s, p2r, p3s, p3r,
    x1s, x1r, x2s, x2r, x3s, x3r, ms, mr, ds, dr, early, weighty, late,
):
    z, y, tp = lax.axis_index("sp_0"), lax.axis_index("sp_1"), lax.axis_index("tp")
    xc, core = tp // 2, tp % 2
    partner = tp + 1 - 2 * core

    def up(at, j, n=8):
        return lax.rem(at + j, n)

    def down(at, j, n=8):
        return lax.rem(at + n - j, n)

    def copy(src, dst, send, recv, axis, at):
        return pltpu.make_async_remote_copy(
            src_ref=src, dst_ref=dst, send_sem=send, recv_sem=recv,
            device_id={axis: at}, device_id_type=MESH,
        )

    barrier = pltpu.get_barrier_semaphore()
    for axis, at in (("sp_0", z), ("sp_1", y), ("tp", tp)):
        for j in range(1, 8):
            pl.semaphore_signal(barrier, inc=1, device_id={axis: up(at, j)}, device_id_type=MESH)

    def fetch(pairs, sem):
        copies = [pltpu.make_async_copy(a, b, sem.at[n]) for n, (a, b) in enumerate(pairs)]
        for c in copies:
            c.start()
        return copies

    early_copies = fetch(
        (
            (key_hbm, key_ref), (fade_hbm, fade_ref), (amend_hbm, amend_ref), (extra_hbm, extra_ref),
            (q_hbm, q_ref), (val_hbm, val_ref),
        ),
        early,
    )
    weight_copies = fetch(
        ((gate_hbm, gate_ref), (wide_hbm, wide_ref), (drow_hbm, drow_ref), (proj_hbm, pb.at[tp])), weighty
    )
    late_copies = fetch(
        (
            (valve_hbm, valve_ref), (bonus_hbm, bonus_ref), (again_hbm, again_ref),
            (skip_hbm, skip_ref), (mgain_hbm, mgain_ref), (cgain_hbm, cgain_ref),
        ),
        late,
    )
    sent = []
    order = (1, 7, 2, 6, 3, 5, 4)

    def go(c):
        c.start()
        sent.append(c)

    for c in early_copies:
        c.wait()
    q, key, val = q_ref[...].astype(F32), key_ref[...].astype(F32), val_ref[...].astype(F32)
    ones = head_ones()
    spread_heads = jnp.where((iota((2, 128), 1) >> 6) == iota((2, 128), 0), 1.0, 0.0).astype(F32)
    inv = lax.rsqrt(dot(key * key, ones) + KEY_EPS)
    sides = []
    for d in range(2):
        k, passed, written, g_all, vw, qc = local_mixer(
            q, key, val, inv, fade_ref[d].astype(F32), amend_ref[d].astype(F32),
            dot(extra_ref[d], spread_heads, 0, 0), d
        )
        passed, written = passed.astype(BF16), written.astype(BF16)
        for part in range(4):
            c1s[4 * d + part] = jnp.concatenate([passed, written[16 * part : 16 * part + 16]], 0)
        sides.append((k, g_all, vw, qc))
    for c in weight_copies:
        c.wait()
    wa[z, y] = jnp.concatenate([gate_ref[:, :640], wide_ref[:, :512]], 1)
    wb[z, y, :, :128] = wide_ref[:, 512:640]
    wb[z, y, :, 128:256] = jnp.concatenate([gate_ref[:, 640:], wide_ref[:, 640:]], 1)
    wb[z, y, :, 256:896] = drow_ref[:, :640]
    wb[z, y, :, 896:] = jnp.concatenate([drow_ref[:, 640:], jnp.zeros((32, 64), BF16)], 1)
    pl.semaphore_wait(barrier, 21)
    for j in order:
        w = up(y, j)
        go(copy(c1s.at[w], c1r.at[y], x1s.at[j - 1], x1r.at[j - 1], "sp_1", w))
    c1r[y] = c1s[y]

    def first_a(j, block, target, part=slice(0, 32), sem=None):
        sem = j - 1 if sem is None else sem
        return copy(wa.at[z, block, part], wa.at[z, block, part], a1s.at[sem], a1r.at[sem], "sp_1", target)

    def first_b(j, block, target, part=slice(0, 32), sem=None):
        sem = j - 1 if sem is None else sem
        return copy(wb.at[block, y, part], wb.at[block, y, part], b1s.at[sem], b1r.at[sem], "sp_0", target)

    for j in (1, 7, 2, 6):
        go(first_a(j, y, up(y, j)))
        go(first_b(j, z, up(z, j)))
    for j in (1, 3, 2):
        go(copy(pb.at[tp], pb.at[tp], p1s.at[j - 1], p1r.at[j - 1], "tp", 2 * up(xc, j, 4) + core))
    go(copy(pb.at[tp], pb.at[tp], p2s.at[0], p2r.at[0], "tp", partner))

    for c in late_copies:
        c.wait()
    reads = []
    for k, g_all, vw, qc in sides:
        oy = bdot(g_all, vw)
        reads.append((oy[:, :128], (qc - oy[:, 128:]).astype(BF16)))
    bonus = dot(q * (sides[0][0] + sides[1][0]) * bonus_ref[...], ones) * val

    for first, at in ((first_a, y), (first_b, z)):
        for j in (1, 7, 2, 6):
            first(j, down(at, j), at).wait_recv()
        go(first(3, down(at, 2), up(at, 1)))
        go(first(5, up(at, 2), down(at, 1)))
        go(first(4, down(at, 2), up(at, 2), slice(0, 16)))
        go(first(4, up(at, 2), down(at, 2), slice(16, 32), 7))

    held = []

    def ring(s, p, start):
        for way in range(2):
            if s == 4 and way != p:
                continue
            back, on = (down, up) if way == 0 else (up, down)
            a_sems = a2s.at[way, s - 1, p], a2r.at[way, s - 1, p]
            b_sems = b2s.at[way, s - 1, p], b2r.at[way, s - 1, p]
            if start:
                n, m = back(z, s - 1), back(y, s - 1)
                for e in PIECES[p]:
                    a, b = wa.at[n, up(y, e)], wb.at[up(z, e), m]
                    copy(a, a, *a_sems, "sp_0", on(z, 1)).start()
                    copy(b, b, *b_sems, "sp_1", on(y, 1)).start()
                held.append(copy(wa.at[0, 0:4], wa.at[0, 0:4], *a_sems, "sp_0", z))
                held.append(copy(wb.at[0, 0:4], wb.at[0, 0:4], *b_sems, "sp_1", y))
            else:
                copy(wa.at[0, 0:4], wa.at[0, 0:4], *a_sems, "sp_0", z).wait_recv()
                copy(wb.at[0, 0:4], wb.at[0, 0:4], *b_sems, "sp_1", y).wait_recv()

    ring(1, 0, True)

    for j in order:
        copy(c1s.at[y], c1r.at[down(y, j)], x1s.at[j - 1], x1r.at[j - 1], "sp_1", y).wait_recv()
    side = y // 4
    both = jnp.where(iota((64, 128), 0) == (iota((64, 128), 1) & 63), 1.0, 0.0).astype(F32)
    joined = jnp.concatenate([both, jnp.zeros((16, 128), F32)], 0)
    fresh = jnp.zeros((64, 128), F32)
    prefixes = []
    for n in range(8):
        prefixes.append(joined)
        block = c1r[n + side * (7 - 2 * n)]
        joined = bdot(joined, expand(block[:64])) + jnp.concatenate(
            [fresh, block[64:].astype(F32)], 0
        )
    c2s[...] = joined.astype(BF16)
    c2r[z] = joined.astype(BF16)
    for j in order:
        go(copy(c2s, c2r.at[z], x2s.at[j - 1], x2r.at[j - 1], "sp_0", up(z, j)))

    for first, at in ((first_a, y), (first_b, z)):
        first(3, down(at, 3), at).wait_recv()
        first(5, up(at, 3), at).wait_recv()
        first(4, up(at, 4), at, slice(0, 16)).wait_recv()
        first(4, up(at, 4), at, slice(16, 32), 7).wait_recv()
    ring(1, 1, True)
    ring(1, 0, False)
    ring(2, 0, True)

    for j in order:
        copy(c2s, c2r.at[down(z, j)], x2s.at[j - 1], x2r.at[j - 1], "sp_0", z).wait_recv()
    entering = jnp.zeros((16, 128), F32)
    for n in range(8):
        at = n + side * (7 - 2 * n)
        block = c2r[at]
        new = bdot(entering, expand(block[:64])) + block[64:].astype(F32)
        before = (1 - 2 * side) * (z - at) > 0
        entering = jnp.where(before, new, entering)
    for n in range(8):
        before = prefixes[n]
        c3s[n + side * (7 - 2 * n)] = (
            bdot(entering, expand(before[:64])) + before[64:]
        ).astype(BF16)
    for j in order:
        w = up(y, j)
        go(copy(c3s.at[w], c3r.at[y], x3s.at[j - 1], x3r.at[j - 1], "sp_1", w))
    c3r[y] = c3s[y]

    for j in (1, 3, 2):
        at = 2 * down(xc, j, 4) + core
        copy(pb.at[tp], pb.at[at], p1s.at[j - 1], p1r.at[j - 1], "tp", tp).wait_recv()
        go(copy(pb.at[at], pb.at[at], p3s.at[j - 1], p3r.at[j - 1], "tp", partner))

    ring(1, 1, False)
    ring(2, 1, True)
    ring(2, 0, False)
    ring(3, 0, True)

    for j in order:
        copy(c3s.at[y], c3r.at[down(y, j)], x3s.at[j - 1], x3r.at[j - 1], "sp_1", y).wait_recv()
    summed = jnp.zeros((64, 128), F32)
    for d in range(2):
        state = jnp.concatenate([c3r[4 * d + part] for part in range(4)], 0)
        summed = summed + reads[d][0] + bdot(reads[d][1], expand(state), 1, 1)
    center = dot(summed, ones) * (1.0 / 64)
    away = summed - center
    spread = dot(away * away, ones) * (1.0 / 64)
    normed = away * lax.rsqrt(spread + GROUP_EPS) * again_ref[...]
    mixed = (normed + bonus) * valve_ref[...].astype(F32)
    mb[tp] = mixed.astype(BF16)
    for j in order:
        go(copy(mb.at[tp], mb.at[tp], ms.at[j - 1], mr.at[j - 1], "tp", up(tp, j)))
    ring(2, 1, False)
    ring(3, 1, True)
    copy(pb.at[tp], pb.at[partner], p2s.at[0], p2r.at[0], "tp", tp).wait_recv()
    for j in (1, 3, 2):
        at = 2 * down(xc, j, 4) + 1 - core
        copy(pb.at[at], pb.at[at], p3s.at[j - 1], p3r.at[j - 1], "tp", tp).wait_recv()
    for j in order:
        copy(mb.at[tp], mb.at[down(tp, j)], ms.at[j - 1], mr.at[j - 1], "tp", tp).wait_recv()

    rows = jnp.concatenate([mb[n] for n in range(8)], 1)

    def project(n, carry):
        cols = pl.ds(pl.multiple_of(n * 256, 256), 256)
        weights = pb[:, :, cols].reshape(1024, 256)
        midf[:, cols] = RESIDUAL_SCALE * skip_ref[:, cols].astype(F32) + bdot(rows, weights)
        return carry

    lax.fori_loop(0, 8, project, 0)

    def layer_norm(x, gain):
        center = jnp.mean(x, -1, keepdims=True)
        away = x - center
        spread = jnp.mean(away * away, -1, keepdims=True)
        return away * lax.rsqrt(spread + NORM_EPS) * gain

    for n in range(8):
        part = slice(8 * n, 8 * n + 8)
        normal = layer_norm(midf[part, :], mgain_ref[...]).astype(BF16)
        midf[part, :] = normal.astype(F32)
    midb[...] = midf[...].astype(BF16)

    ring(3, 0, False)
    ring(4, 0, True)
    ring(3, 1, False)
    ring(4, 1, True)

    gu[...] = jnp.zeros_like(gu)

    def widen(n):
        mid = midb[:, pl.ds(pl.multiple_of(n * 256, 256), 256)]
        gu[:, :1152] += bdot(mid, wa[n].reshape(256, 1152))

    def widen_near(n, carry):
        widen(up(z, n + 5))
        return carry

    def widen_rest(n, carry):
        mid = midb[:, pl.ds(pl.multiple_of(n * 256, 256), 256)]
        gu[:, 1152:] += bdot(mid, wb[n, :, :, :256].reshape(256, 256))
        return carry

    lax.fori_loop(0, 7, widen_near, 0)
    ring(4, 0, False)
    ring(4, 1, False)
    widen(up(z, 4))
    lax.fori_loop(0, 8, widen_rest, 0)

    gate, wide = gu[:, :640], gu[:, 640:1280]
    tail = gu[:, 1280:]
    main = gate / (1.0 + jnp.exp(-gate)) * wide
    rest = tail / (1.0 + jnp.exp(-tail)) * pltpu.roll(tail, 64, 1)
    rest = jnp.where(iota((64, 128), 1) < 64, rest, 0.0)
    inner = jnp.concatenate([main, rest], 1).astype(BF16)

    def shrink(n, carry):
        cols = pl.ds(pl.multiple_of(n * 256, 256), 256)
        share = bdot(inner, wb[n, :, :, 256:].reshape(256, 768), 1, 1)
        for m in range(8):
            rs[m, :, cols] = share[8 * m : 8 * m + 8].astype(BF16)
        return carry

    lax.fori_loop(0, 8, shrink, 0)
    for j in order:
        go(copy(rs.at[up(tp, j)], rr.at[tp], ds.at[j - 1], dr.at[j - 1], "tp", up(tp, j)))
    rr[tp] = rs[tp]
    for j in order:
        copy(rs.at[tp], rr.at[down(tp, j)], ds.at[j - 1], dr.at[j - 1], "tp", tp).wait_recv()
    total = RESIDUAL_SCALE * midf[pl.ds(pl.multiple_of(tp * 8, 8), 8), :]
    for n in range(8):
        total = total + rr[n].astype(F32)
    out_ref[...] = layer_norm(total, cgain_ref[...]).astype(BF16)
    for c in sent + held:
        c.wait_send()


def shards(
    skip, reading, labels, payloads, valve, fading, amend, extra, bonus, again, projector,
    mgain, gate, wide, shrink, cgain,
):
    down_rows = jnp.swapaxes(shrink, 0, 1)
    dma = pltpu.SemaphoreType.DMA
    sems = [(8,)] * 4 + [(2, 4, 2)] * 4 + [(3,), (3,), (1,), (1,), (3,), (3,)] + [(7,)] * 10 + [(6,), (4,), (6,)]
    return pl.pallas_call(
        body,
        out_shape=jax.ShapeDtypeStruct((8, 2048), BF16),
        in_specs=[pl.BlockSpec(memory_space=pltpu.HBM)] * 16,
        out_specs=pl.BlockSpec(memory_space=pltpu.VMEM),
        scratch_shapes=[
            pltpu.VMEM((64, 2048), BF16),
            pltpu.VMEM((64, 128), BF16),
            pltpu.VMEM((64, 128), BF16),
            pltpu.VMEM((64, 128), BF16),
            pltpu.VMEM((64, 128), BF16),
            pltpu.VMEM((2, 64, 128), BF16),
            pltpu.VMEM((2, 64, 128), BF16),
            pltpu.VMEM((2, 2, 64), F32),
            pltpu.VMEM((1, 128), F32),
            pltpu.VMEM((1, 128), F32),
            pltpu.VMEM((1, 2048), F32),
            pltpu.VMEM((32, 704), BF16),
            pltpu.VMEM((32, 704), BF16),
            pltpu.VMEM((32, 704), BF16),
            pltpu.VMEM((1, 2048), F32),
            pltpu.VMEM((8, 8, 32, WA_COLS), BF16),
            pltpu.VMEM((8, 8, 32, WB_COLS), BF16),
            pltpu.VMEM((8, 128, 2048), BF16),
            pltpu.VMEM((8, 80, 128), BF16),
            pltpu.VMEM((8, 80, 128), BF16),
            pltpu.VMEM((80, 128), BF16),
            pltpu.VMEM((8, 80, 128), BF16),
            pltpu.VMEM((8, 16, 128), BF16),
            pltpu.VMEM((8, 16, 128), BF16),
            pltpu.VMEM((8, 64, 128), BF16),
            pltpu.VMEM((8, 8, 2048), BF16),
            pltpu.VMEM((8, 8, 2048), BF16),
            pltpu.VMEM((64, 2048), F32),
            pltpu.VMEM((64, 2048), BF16),
            pltpu.VMEM((64, 1408), F32),
        ]
        + [dma(s) for s in sems],
        compiler_params=pltpu.CompilerParams(
            collective_id=0, has_side_effects=True, vmem_limit_bytes=67043328
        ),
    )(
        skip, reading, labels, payloads, valve, fading, amend, extra, bonus.reshape(1, 128),
        again.reshape(1, 128), projector, mgain.reshape(1, 2048), gate, wide,
        down_rows, cgain.reshape(1, 2048),
    )


def solution(mesh):
    finer = Mesh(mesh.devices.reshape(8, 8, mesh.shape["tp"]), ("sp_0", "sp_1", "tp"))
    placed = (
        P(SP, None),
        P(SP, "tp"),
        P(SP, "tp"),
        P(SP, "tp"),
        P(SP, "tp"),
        P(None, SP, "tp"),
        P(None, SP, "tp"),
        P(None, "tp", SP),
        P("tp"),
        P("tp"),
        P("tp", None),
        P(),
        P(SP, "tp"),
        P(SP, "tp"),
        P("tp", SP),
        P(),
    )
    return jax.shard_map(
        shards, mesh=finer, in_specs=placed, out_specs=P(SP_TP, None), check_vma=False
    )
```

```python
import jax
import jax.numpy as jnp
from jax import lax
from jax.experimental import pallas as pl
from jax.experimental.pallas import tpu as pltpu
from jax.sharding import Mesh
from jax.sharding import PartitionSpec as P

SP = ("sp_0", "sp_1")
SP_TP = ("sp_0", "sp_1", "tp")
MESH = pl.DeviceIdType.MESH
F32 = jnp.float32
BF16 = jnp.bfloat16
HIGHEST = lax.Precision.HIGHEST

RESIDUAL_SCALE = 2.0**0.25
NORM_EPS = 1e-05
GROUP_EPS = 0.00064
KEY_EPS = 1e-06
HALF_EXP = 0.6065306597126334

TOK = 64
LANES = 128
WA_COLS = 1152
WB_COLS = 1024
PIECES = ((0, 1, 7), (2, 6), (3, 5, 4))


def dot(a, b, ca=1, cb=0):
    return lax.dot_general(
        a, b, (((ca,), (cb,)), ((), ())), precision=HIGHEST, preferred_element_type=F32
    )


def bdot(a, b, ca=1, cb=0):
    return lax.dot_general(
        a.astype(BF16), b.astype(BF16), (((ca,), (cb,)), ((), ())), preferred_element_type=F32
    )


def iota(shape, dim):
    return lax.broadcasted_iota(jnp.int32, shape, dim)


def expand(x):
    lane = iota(x.shape, 1)
    zero = jnp.zeros_like(x)
    return jnp.concatenate([jnp.where(lane < 64, x, zero), jnp.where(lane >= 64, x, zero)], 0)


def fold(z):
    half = z.shape[0] // 2
    return z[:half] + z[half:]


def head_ones():
    return jnp.where((iota((128, 128), 0) < 64) == (iota((128, 128), 1) < 64), 1.0, 0.0).astype(F32)


def local_mixer(q, key, val, inv, fade, amend, extra, d):
    row, col = iota((64, 64), 0), iota((64, 64), 1)
    k = key * jax.nn.sigmoid(amend)
    logw = extra - jax.nn.sigmoid(fade) * HALF_EXP
    tri = jnp.where(col <= row if d == 0 else col >= row, 1.0, 0.0).astype(F32)
    c = dot(tri, logw)
    cx = c - logw
    end = c[63:64] if d == 0 else c[0:1]
    un = key * inv * inv
    erase_rows, read_rows = [], []
    for i in range(4):
        lo = 16 * i
        ref = cx[lo : lo + 1] if d == 0 else cx[lo + 15 : lo + 16]
        kk = k * jnp.exp(jnp.minimum(ref - c, 60.0))
        lu = un[lo : lo + 16] * jnp.exp(cx[lo : lo + 16] - ref)
        lq = q[lo : lo + 16] * jnp.exp(c[lo : lo + 16] - ref)
        res = bdot(jnp.concatenate([lu, lq], 0), expand(kk), 1, 1)
        erase_rows.append(res[:16])
        read_rows.append(res[16:])
    m_all = jnp.concatenate(erase_rows, 0)
    g_all = jnp.concatenate(read_rows, 0)
    rt, ct = iota((64, 128), 0), iota((64, 128), 1) & 63
    m_all = expand(jnp.where(ct < rt if d == 0 else ct > rt, m_all, 0.0))
    g_all = jnp.where(ct <= rt if d == 0 else ct >= rt, g_all, 0.0)
    r, cc = iota((128, 128), 0), iota((128, 128), 1)
    eye = jnp.where(r == cc, 1.0, 0.0).astype(F32)
    inverse = eye - jnp.where((r >> 1) == (cc >> 1), m_all, 0.0)
    for b in range(1, 6):
        off = jnp.where(((r >> (b + 1)) == (cc >> (b + 1))) & ((r >> b) != (cc >> b)), m_all, 0.0)
        inverse = inverse - dot(dot(inverse, off), inverse)
    ut = un * jnp.exp(cx)
    vw = dot(inverse, jnp.concatenate([expand(val), expand(ut)], 1))
    kend = expand(k * jnp.exp(end - c))
    z = bdot(vw, kend, 0, 0)
    written = fold(z[:128])
    passed = jnp.where(rt == ct, jnp.exp(end), 0.0) - fold(z[128:])
    return k, passed, written, g_all, vw, q * jnp.exp(c)


def body(
    skip_hbm, q_hbm, key_hbm, val_hbm, valve_hbm, fade_hbm, amend_hbm, extra_hbm, bonus_hbm,
    again_hbm, proj_hbm, mgain_hbm, gate_hbm, wide_hbm, drow_hbm, cgain_hbm, out_ref,
    skip_ref, q_ref, key_ref, val_ref, valve_ref, fade_ref, amend_ref, extra_ref, bonus_ref,
    again_ref, mgain_ref, gate_ref, wide_ref, drow_ref, cgain_ref,
    wa, wb, pb, c1s, c1r, c2s, c2r, c3s, c3r, mb, rs, rr, midf, midb, gu,
    a1s, a1r, b1s, b1r, a2s, a2r, b2s, b2r, p1s, p1r, p2s, p2r, p3s, p3r,
    x1s, x1r, x2s, x2r, x3s, x3r, ms, mr, ds, dr, early, weighty, late,
):
    z, y, tp = lax.axis_index("sp_0"), lax.axis_index("sp_1"), lax.axis_index("tp")
    xc, core = tp // 2, tp % 2
    partner = tp + 1 - 2 * core

    def up(at, j, n=8):
        return lax.rem(at + j, n)

    def down(at, j, n=8):
        return lax.rem(at + n - j, n)

    def copy(src, dst, send, recv, axis, at):
        return pltpu.make_async_remote_copy(
            src_ref=src, dst_ref=dst, send_sem=send, recv_sem=recv,
            device_id={axis: at}, device_id_type=MESH,
        )

    barrier = pltpu.get_barrier_semaphore()
    for axis, at in (("sp_0", z), ("sp_1", y), ("tp", tp)):
        for j in range(1, 8):
            pl.semaphore_signal(barrier, inc=1, device_id={axis: up(at, j)}, device_id_type=MESH)

    def fetch(pairs, sem):
        copies = [pltpu.make_async_copy(a, b, sem.at[n]) for n, (a, b) in enumerate(pairs)]
        for c in copies:
            c.start()
        return copies

    early_copies = fetch(
        (
            (key_hbm, key_ref), (fade_hbm, fade_ref), (amend_hbm, amend_ref), (extra_hbm, extra_ref),
            (q_hbm, q_ref), (val_hbm, val_ref),
        ),
        early,
    )
    weight_copies = fetch(
        ((gate_hbm, gate_ref), (wide_hbm, wide_ref), (drow_hbm, drow_ref), (proj_hbm, pb.at[tp])), weighty
    )
    late_copies = fetch(
        (
            (valve_hbm, valve_ref), (bonus_hbm, bonus_ref), (again_hbm, again_ref),
            (skip_hbm, skip_ref), (mgain_hbm, mgain_ref), (cgain_hbm, cgain_ref),
        ),
        late,
    )
    sent = []
    order = (1, 7, 2, 6, 3, 5, 4)

    def go(c):
        c.start()
        sent.append(c)

    for c in early_copies:
        c.wait()
    q, key, val = q_ref[...].astype(F32), key_ref[...].astype(F32), val_ref[...].astype(F32)
    ones = head_ones()
    spread_heads = jnp.where((iota((2, 128), 1) >> 6) == iota((2, 128), 0), 1.0, 0.0).astype(F32)
    inv = lax.rsqrt(dot(key * key, ones) + KEY_EPS)
    sides = []
    for d in range(2):
        k, passed, written, g_all, vw, qc = local_mixer(
            q, key, val, inv, fade_ref[d].astype(F32), amend_ref[d].astype(F32),
            dot(extra_ref[d], spread_heads, 0, 0), d
        )
        passed, written = passed.astype(BF16), written.astype(BF16)
        for part in range(4):
            c1s[4 * d + part] = jnp.concatenate([passed, written[16 * part : 16 * part + 16]], 0)
        sides.append((k, g_all, vw, qc))
    for c in weight_copies:
        c.wait()
    wa[z, y] = jnp.concatenate([gate_ref[:, :640], wide_ref[:, :512]], 1)
    wb[z, y, :, :128] = wide_ref[:, 512:640]
    wb[z, y, :, 128:256] = jnp.concatenate([gate_ref[:, 640:], wide_ref[:, 640:]], 1)
    wb[z, y, :, 256:896] = drow_ref[:, :640]
    wb[z, y, :, 896:] = jnp.concatenate([drow_ref[:, 640:], jnp.zeros((32, 64), BF16)], 1)
    pl.semaphore_wait(barrier, 21)
    def first(k, start):
        for way in range(2):
            back, on = (down, up) if way == 0 else (up, down)
            part = slice(0, 32) if k < 4 else slice(16 * way, 16 * way + 16)
            at = k - 1 if start else k
            a, b = wa.at[z, back(y, at), part], wb.at[back(z, at), y, part]
            a = copy(a, a, a1s.at[way, k - 1], a1r.at[way, k - 1], "sp_1", on(y, 1))
            b = copy(b, b, b1s.at[way, k - 1], b1r.at[way, k - 1], "sp_0", on(z, 1))
            if start:
                go(a)
                go(b)
            else:
                a.wait_recv()
                b.wait_recv()

    held = []

    def piece(s, p, way):
        if s < 4:
            return PIECES[p]
        return (((0, 1, 7), (2,), ()), ((), (6,), (3, 5, 4)))[way][p]

    def ring_sems(s, p, way):
        return (a2s.at[way, s - 1, p], a2r.at[way, s - 1, p]), (b2s.at[way, s - 1, p], b2r.at[way, s - 1, p])

    def whole(s, p, way):
        n = len(piece(s, p, way))
        a_sems, b_sems = ring_sems(s, p, way)
        return (
            copy(wa.at[0, 0:n], wa.at[0, 0:n], *a_sems, "sp_0", z),
            copy(wb.at[0, 0:n], wb.at[0, 0:n], *b_sems, "sp_1", y),
        )

    def send(s, p, only=None):
        for way in range(2):
            back, on = (down, up) if way == 0 else (up, down)
            a_sems, b_sems = ring_sems(s, p, way)
            n, m = back(z, s - 1), back(y, s - 1)
            for e in piece(s, p, way) if only is None else only:
                a, b = wa.at[n, up(y, e)], wb.at[up(z, e), m]
                copy(a, a, *a_sems, "sp_0", on(z, 1)).start()
                copy(b, b, *b_sems, "sp_1", on(y, 1)).start()
            if piece(s, p, way) and (only is None or only[-1] == PIECES[p][-1]):
                held.extend(whole(s, p, way))

    def take(s, p):
        for way in range(2):
            if piece(s, p, way):
                for c in whole(s, p, way):
                    c.wait_recv()

    first(1, True)
    send(1, 0, (0,))
    for j in order:
        w = up(y, j)
        go(copy(c1s.at[w], c1r.at[y], x1s.at[j - 1], x1r.at[j - 1], "sp_1", w))
    c1r[y] = c1s[y]
    for j in (1, 3, 2):
        go(copy(pb.at[tp], pb.at[tp], p1s.at[j - 1], p1r.at[j - 1], "tp", 2 * up(xc, j, 4) + core))
    go(copy(pb.at[tp], pb.at[tp], p2s.at[0], p2r.at[0], "tp", partner))

    first(1, False)
    first(2, True)
    send(1, 0, (1, 7))

    for c in late_copies:
        c.wait()
    reads = []
    for k, g_all, vw, qc in sides:
        oy = bdot(g_all, vw)
        reads.append((oy[:, :128], (qc - oy[:, 128:]).astype(BF16)))
    bonus = dot(q * (sides[0][0] + sides[1][0]) * bonus_ref[...], ones) * val

    first(2, False)
    first(3, True)
    send(1, 1)

    for j in order:
        copy(c1s.at[y], c1r.at[down(y, j)], x1s.at[j - 1], x1r.at[j - 1], "sp_1", y).wait_recv()
    side = y // 4
    both = jnp.where(iota((64, 128), 0) == (iota((64, 128), 1) & 63), 1.0, 0.0).astype(F32)
    joined = jnp.concatenate([both, jnp.zeros((16, 128), F32)], 0)
    fresh = jnp.zeros((64, 128), F32)
    prefixes = []
    for n in range(8):
        prefixes.append(joined)
        block = c1r[n + side * (7 - 2 * n)]
        joined = bdot(joined, expand(block[:64])) + jnp.concatenate(
            [fresh, block[64:].astype(F32)], 0
        )
    c2s[...] = joined.astype(BF16)
    c2r[z] = joined.astype(BF16)
    for j in order:
        go(copy(c2s, c2r.at[z], x2s.at[j - 1], x2r.at[j - 1], "sp_0", up(z, j)))

    first(3, False)
    first(4, True)
    send(1, 2, (3, 5))
    take(1, 0)
    send(2, 0)
    first(4, False)
    send(1, 2, (4,))
    take(1, 1)
    send(2, 1)

    for j in order:
        copy(c2s, c2r.at[down(z, j)], x2s.at[j - 1], x2r.at[j - 1], "sp_0", z).wait_recv()
    entering = jnp.zeros((16, 128), F32)
    for n in range(8):
        at = n + side * (7 - 2 * n)
        block = c2r[at]
        new = bdot(entering, expand(block[:64])) + block[64:].astype(F32)
        before = (1 - 2 * side) * (z - at) > 0
        entering = jnp.where(before, new, entering)
    for n in range(8):
        before = prefixes[n]
        c3s[n + side * (7 - 2 * n)] = (
            bdot(entering, expand(before[:64])) + before[64:]
        ).astype(BF16)
    for j in order:
        w = up(y, j)
        go(copy(c3s.at[w], c3r.at[y], x3s.at[j - 1], x3r.at[j - 1], "sp_1", w))
    c3r[y] = c3s[y]

    take(1, 2)
    send(2, 2)
    take(2, 0)
    send(3, 0)

    for j in (1, 3, 2):
        at = 2 * down(xc, j, 4) + core
        copy(pb.at[tp], pb.at[at], p1s.at[j - 1], p1r.at[j - 1], "tp", tp).wait_recv()
        go(copy(pb.at[at], pb.at[at], p3s.at[j - 1], p3r.at[j - 1], "tp", partner))

    take(2, 1)
    send(3, 1)

    for j in order:
        copy(c3s.at[y], c3r.at[down(y, j)], x3s.at[j - 1], x3r.at[j - 1], "sp_1", y).wait_recv()
    summed = jnp.zeros((64, 128), F32)
    for d in range(2):
        state = jnp.concatenate([c3r[4 * d + part] for part in range(4)], 0)
        summed = summed + reads[d][0] + bdot(reads[d][1], expand(state), 1, 1)
    center = dot(summed, ones) * (1.0 / 64)
    away = summed - center
    spread = dot(away * away, ones) * (1.0 / 64)
    normed = away * lax.rsqrt(spread + GROUP_EPS) * again_ref[...]
    mixed = (normed + bonus) * valve_ref[...].astype(F32)
    mb[tp] = mixed.astype(BF16)
    for j in order:
        go(copy(mb.at[tp], mb.at[tp], ms.at[j - 1], mr.at[j - 1], "tp", up(tp, j)))
    take(2, 2)
    send(3, 2)
    copy(pb.at[tp], pb.at[partner], p2s.at[0], p2r.at[0], "tp", tp).wait_recv()
    for j in (1, 3, 2):
        at = 2 * down(xc, j, 4) + 1 - core
        copy(pb.at[at], pb.at[at], p3s.at[j - 1], p3r.at[j - 1], "tp", tp).wait_recv()
    for j in order:
        copy(mb.at[tp], mb.at[down(tp, j)], ms.at[j - 1], mr.at[j - 1], "tp", tp).wait_recv()

    rows = jnp.concatenate([mb[n] for n in range(8)], 1)

    def project(n, carry):
        cols = pl.ds(pl.multiple_of(n * 256, 256), 256)
        weights = pb[:, :, cols].reshape(1024, 256)
        midf[:, cols] = RESIDUAL_SCALE * skip_ref[:, cols].astype(F32) + bdot(rows, weights)
        return carry

    lax.fori_loop(0, 8, project, 0)

    def layer_norm(x, gain):
        center = jnp.mean(x, -1, keepdims=True)
        away = x - center
        spread = jnp.mean(away * away, -1, keepdims=True)
        return away * lax.rsqrt(spread + NORM_EPS) * gain

    for n in range(8):
        part = slice(8 * n, 8 * n + 8)
        normal = layer_norm(midf[part, :], mgain_ref[...]).astype(BF16)
        midf[part, :] = normal.astype(F32)
    midb[...] = midf[...].astype(BF16)

    take(3, 0)
    send(4, 0)
    take(3, 1)
    send(4, 1)
    take(3, 2)
    send(4, 2)

    gu[...] = jnp.zeros_like(gu)

    def widen(n):
        mid = midb[:, pl.ds(pl.multiple_of(n * 256, 256), 256)]
        gu[:, :1152] += bdot(mid, wa[n].reshape(256, 1152))

    def widen_near(n, carry):
        widen(up(z, n + 5))
        return carry

    def widen_rest(n, carry):
        mid = midb[:, pl.ds(pl.multiple_of(n * 256, 256), 256)]
        gu[:, 1152:] += bdot(mid, wb[n, :, :, :256].reshape(256, 256))
        return carry

    lax.fori_loop(0, 7, widen_near, 0)
    take(4, 0)
    take(4, 1)
    take(4, 2)
    widen(up(z, 4))
    lax.fori_loop(0, 8, widen_rest, 0)

    gate, wide = gu[:, :640], gu[:, 640:1280]
    tail = gu[:, 1280:]
    main = gate / (1.0 + jnp.exp(-gate)) * wide
    rest = tail / (1.0 + jnp.exp(-tail)) * pltpu.roll(tail, 64, 1)
    rest = jnp.where(iota((64, 128), 1) < 64, rest, 0.0)
    inner = jnp.concatenate([main, rest], 1).astype(BF16)

    def shrink(n, carry):
        cols = pl.ds(pl.multiple_of(n * 256, 256), 256)
        share = bdot(inner, wb[n, :, :, 256:].reshape(256, 768), 1, 1)
        for m in range(8):
            rs[m, :, cols] = share[8 * m : 8 * m + 8].astype(BF16)
        return carry

    def share_copy(half, j, source, target):
        cols = slice(1024 * half, 1024 * half + 1024)
        return copy(
            rs.at[target, :, cols], rr.at[source, :, cols], ds.at[half, j - 1], dr.at[half, j - 1], "tp", target
        )

    for half in range(2):
        lax.fori_loop(4 * half, 4 * half + 4, shrink, 0)
        for j in order:
            go(share_copy(half, j, tp, up(tp, j)))
    rr[tp] = rs[tp]
    for half in range(2):
        for j in order:
            share_copy(half, j, down(tp, j), tp).wait_recv()
    total = RESIDUAL_SCALE * midf[pl.ds(pl.multiple_of(tp * 8, 8), 8), :]
    for n in range(8):
        total = total + rr[n].astype(F32)
    out_ref[...] = layer_norm(total, cgain_ref[...]).astype(BF16)
    for c in sent + held:
        c.wait_send()


def shards(
    skip, reading, labels, payloads, valve, fading, amend, extra, bonus, again, projector,
    mgain, gate, wide, shrink, cgain,
):
    down_rows = jnp.swapaxes(shrink, 0, 1)
    dma = pltpu.SemaphoreType.DMA
    sems = [(2, 4)] * 4 + [(2, 4, 3)] * 4 + [(3,), (3,), (1,), (1,), (3,), (3,)] + [(7,)] * 8 + [(2, 7)] * 2 + [(6,), (4,), (6,)]
    return pl.pallas_call(
        body,
        out_shape=jax.ShapeDtypeStruct((8, 2048), BF16),
        in_specs=[pl.BlockSpec(memory_space=pltpu.HBM)] * 16,
        out_specs=pl.BlockSpec(memory_space=pltpu.VMEM),
        scratch_shapes=[
            pltpu.VMEM((64, 2048), BF16),
            pltpu.VMEM((64, 128), BF16),
            pltpu.VMEM((64, 128), BF16),
            pltpu.VMEM((64, 128), BF16),
            pltpu.VMEM((64, 128), BF16),
            pltpu.VMEM((2, 64, 128), BF16),
            pltpu.VMEM((2, 64, 128), BF16),
            pltpu.VMEM((2, 2, 64), F32),
            pltpu.VMEM((1, 128), F32),
            pltpu.VMEM((1, 128), F32),
            pltpu.VMEM((1, 2048), F32),
            pltpu.VMEM((32, 704), BF16),
            pltpu.VMEM((32, 704), BF16),
            pltpu.VMEM((32, 704), BF16),
            pltpu.VMEM((1, 2048), F32),
            pltpu.VMEM((8, 8, 32, WA_COLS), BF16),
            pltpu.VMEM((8, 8, 32, WB_COLS), BF16),
            pltpu.VMEM((8, 128, 2048), BF16),
            pltpu.VMEM((8, 80, 128), BF16),
            pltpu.VMEM((8, 80, 128), BF16),
            pltpu.VMEM((80, 128), BF16),
            pltpu.VMEM((8, 80, 128), BF16),
            pltpu.VMEM((8, 16, 128), BF16),
            pltpu.VMEM((8, 16, 128), BF16),
            pltpu.VMEM((8, 64, 128), BF16),
            pltpu.VMEM((8, 8, 2048), BF16),
            pltpu.VMEM((8, 8, 2048), BF16),
            pltpu.VMEM((64, 2048), F32),
            pltpu.VMEM((64, 2048), BF16),
            pltpu.VMEM((64, 1408), F32),
        ]
        + [dma(s) for s in sems],
        compiler_params=pltpu.CompilerParams(
            collective_id=0, has_side_effects=True, vmem_limit_bytes=67043328
        ),
    )(
        skip, reading, labels, payloads, valve, fading, amend, extra, bonus.reshape(1, 128),
        again.reshape(1, 128), projector, mgain.reshape(1, 2048), gate, wide,
        down_rows, cgain.reshape(1, 2048),
    )


def solution(mesh):
    finer = Mesh(mesh.devices.reshape(8, 8, mesh.shape["tp"]), ("sp_0", "sp_1", "tp"))
    placed = (
        P(SP, None),
        P(SP, "tp"),
        P(SP, "tp"),
        P(SP, "tp"),
        P(SP, "tp"),
        P(None, SP, "tp"),
        P(None, SP, "tp"),
        P(None, "tp", SP),
        P("tp"),
        P("tp"),
        P("tp", None),
        P(),
        P(SP, "tp"),
        P(SP, "tp"),
        P("tp", SP),
        P(),
    )
    return jax.shard_map(
        shards, mesh=finer, in_specs=placed, out_specs=P(SP_TP, None), check_vma=False
    )
```

```python
import jax
import jax.numpy as jnp
from jax import lax
from jax.experimental import pallas as pl
from jax.experimental.pallas import tpu as pltpu
from jax.sharding import Mesh
from jax.sharding import PartitionSpec as P

SP = ("sp_0", "sp_1")
SP_TP = ("sp_0", "sp_1", "tp")
MESH = pl.DeviceIdType.MESH
F32 = jnp.float32
BF16 = jnp.bfloat16
HIGHEST = lax.Precision.HIGHEST

RESIDUAL_SCALE = 2.0**0.25
NORM_EPS = 1e-05
GROUP_EPS = 0.00064
KEY_EPS = 1e-06
HALF_EXP = 0.6065306597126334

TOK = 64
LANES = 128
WA_COLS = 1152
WB_COLS = 1024
PIECES = ((0, 1, 7), (2, 6), (3, 5, 4))


def dot(a, b, ca=1, cb=0):
    return lax.dot_general(
        a, b, (((ca,), (cb,)), ((), ())), precision=HIGHEST, preferred_element_type=F32
    )


def bdot(a, b, ca=1, cb=0):
    return lax.dot_general(
        a.astype(BF16), b.astype(BF16), (((ca,), (cb,)), ((), ())), preferred_element_type=F32
    )


def iota(shape, dim):
    return lax.broadcasted_iota(jnp.int32, shape, dim)


def expand(x):
    lane = iota(x.shape, 1)
    zero = jnp.zeros_like(x)
    return jnp.concatenate([jnp.where(lane < 64, x, zero), jnp.where(lane >= 64, x, zero)], 0)


def fold(z):
    half = z.shape[0] // 2
    return z[:half] + z[half:]


def head_ones():
    return jnp.where((iota((128, 128), 0) < 64) == (iota((128, 128), 1) < 64), 1.0, 0.0).astype(F32)


def local_mixer(q, key, val, inv, fade, amend, extra, d):
    row, col = iota((64, 64), 0), iota((64, 64), 1)
    k = key * jax.nn.sigmoid(amend)
    logw = extra - jax.nn.sigmoid(fade) * HALF_EXP
    tri = jnp.where(col <= row if d == 0 else col >= row, 1.0, 0.0).astype(F32)
    c = dot(tri, logw)
    cx = c - logw
    end = c[63:64] if d == 0 else c[0:1]
    un = key * inv * inv
    erase_rows, read_rows = [], []
    for i in range(4):
        lo = 16 * i
        ref = cx[lo : lo + 1] if d == 0 else cx[lo + 15 : lo + 16]
        kk = k * jnp.exp(jnp.minimum(ref - c, 60.0))
        lu = un[lo : lo + 16] * jnp.exp(cx[lo : lo + 16] - ref)
        lq = q[lo : lo + 16] * jnp.exp(c[lo : lo + 16] - ref)
        res = bdot(jnp.concatenate([lu, lq], 0), expand(kk), 1, 1)
        erase_rows.append(res[:16])
        read_rows.append(res[16:])
    m_all = jnp.concatenate(erase_rows, 0)
    g_all = jnp.concatenate(read_rows, 0)
    rt, ct = iota((64, 128), 0), iota((64, 128), 1) & 63
    m_all = expand(jnp.where(ct < rt if d == 0 else ct > rt, m_all, 0.0))
    g_all = jnp.where(ct <= rt if d == 0 else ct >= rt, g_all, 0.0)
    r, cc = iota((128, 128), 0), iota((128, 128), 1)
    eye = jnp.where(r == cc, 1.0, 0.0).astype(F32)
    inverse = eye - jnp.where((r >> 1) == (cc >> 1), m_all, 0.0)
    for b in range(1, 6):
        off = jnp.where(((r >> (b + 1)) == (cc >> (b + 1))) & ((r >> b) != (cc >> b)), m_all, 0.0)
        inverse = inverse - dot(dot(inverse, off), inverse)
    ut = un * jnp.exp(cx)
    vw = dot(inverse, jnp.concatenate([expand(val), expand(ut)], 1))
    kend = expand(k * jnp.exp(end - c))
    z = bdot(vw, kend, 0, 0)
    written = fold(z[:128])
    passed = jnp.where(rt == ct, jnp.exp(end), 0.0) - fold(z[128:])
    return k, passed, written, g_all, vw, q * jnp.exp(c)


def body(
    skip_hbm, q_hbm, key_hbm, val_hbm, valve_hbm, fade_hbm, amend_hbm, extra_hbm, bonus_hbm,
    again_hbm, proj_hbm, mgain_hbm, gate_hbm, wide_hbm, drow_hbm, cgain_hbm, out_ref,
    skip_ref, q_ref, key_ref, val_ref, valve_ref, fade_ref, amend_ref, extra_ref, bonus_ref,
    again_ref, mgain_ref, gate_ref, wide_ref, drow_ref, cgain_ref,
    wa, wb, pb, c1s, c1r, c2s, c2r, c3s, c3r, mb, rs, rr, midf, midb, gu,
    a1s, a1r, b1s, b1r, a2s, a2r, b2s, b2r, p1s, p1r, p2s, p2r, p3s, p3r,
    x1s, x1r, x2s, x2r, x3s, x3r, ms, mr, ds, dr, early, weighty, late,
):
    z, y, tp = lax.axis_index("sp_0"), lax.axis_index("sp_1"), lax.axis_index("tp")
    xc, core = tp // 2, tp % 2
    partner = tp + 1 - 2 * core

    def up(at, j, n=8):
        return lax.rem(at + j, n)

    def down(at, j, n=8):
        return lax.rem(at + n - j, n)

    def copy(src, dst, send, recv, axis, at):
        return pltpu.make_async_remote_copy(
            src_ref=src, dst_ref=dst, send_sem=send, recv_sem=recv,
            device_id={axis: at}, device_id_type=MESH,
        )

    barrier = pltpu.get_barrier_semaphore()
    for axis, at in (("sp_0", z), ("sp_1", y), ("tp", tp)):
        for j in range(1, 8):
            pl.semaphore_signal(barrier, inc=1, device_id={axis: up(at, j)}, device_id_type=MESH)

    def fetch(pairs, sem):
        copies = [pltpu.make_async_copy(a, b, sem.at[n]) for n, (a, b) in enumerate(pairs)]
        for c in copies:
            c.start()
        return copies

    early_copies = fetch(
        (
            (key_hbm, key_ref), (fade_hbm, fade_ref), (amend_hbm, amend_ref), (extra_hbm, extra_ref),
            (q_hbm, q_ref), (val_hbm, val_ref),
        ),
        early,
    )
    weight_copies = fetch(
        ((gate_hbm, gate_ref), (wide_hbm, wide_ref), (drow_hbm, drow_ref), (proj_hbm, pb.at[tp])), weighty
    )
    late_copies = fetch(
        (
            (valve_hbm, valve_ref), (bonus_hbm, bonus_ref), (again_hbm, again_ref),
            (skip_hbm, skip_ref), (mgain_hbm, mgain_ref), (cgain_hbm, cgain_ref),
        ),
        late,
    )
    sent = []
    order = (1, 7, 2, 6, 3, 5, 4)

    def go(c):
        c.start()
        sent.append(c)

    for c in early_copies:
        c.wait()
    q, key, val = q_ref[...].astype(F32), key_ref[...].astype(F32), val_ref[...].astype(F32)
    ones = head_ones()
    spread_heads = jnp.where((iota((2, 128), 1) >> 6) == iota((2, 128), 0), 1.0, 0.0).astype(F32)
    inv = lax.rsqrt(dot(key * key, ones) + KEY_EPS)
    for c in weight_copies:
        c.wait()
    wa[z, y] = jnp.concatenate([gate_ref[:, :640], wide_ref[:, :512]], 1)
    wb[z, y, :, :128] = wide_ref[:, 512:640]
    wb[z, y, :, 128:256] = jnp.concatenate([gate_ref[:, 640:], wide_ref[:, 640:]], 1)
    wb[z, y, :, 256:896] = drow_ref[:, :640]
    wb[z, y, :, 896:] = jnp.concatenate([drow_ref[:, 640:], jnp.zeros((32, 64), BF16)], 1)
    def first(k, start):
        for way in range(2):
            back, on = (down, up) if way == 0 else (up, down)
            part = slice(0, 32) if k < 4 else slice(16 * way, 16 * way + 16)
            at = k - 1 if start else k
            a, b = wa.at[z, back(y, at), part], wb.at[back(z, at), y, part]
            a = copy(a, a, a1s.at[way, k - 1], a1r.at[way, k - 1], "sp_1", on(y, 1))
            b = copy(b, b, b1s.at[way, k - 1], b1r.at[way, k - 1], "sp_0", on(z, 1))
            if start:
                go(a)
                go(b)
            else:
                a.wait_recv()
                b.wait_recv()

    held = []

    def piece(s, p, way):
        if s < 4:
            return PIECES[p]
        return (((0, 1, 7), (2,), ()), ((), (6,), (3, 5, 4)))[way][p]

    def ring_sems(s, p, way):
        return (a2s.at[way, s - 1, p], a2r.at[way, s - 1, p]), (b2s.at[way, s - 1, p], b2r.at[way, s - 1, p])

    def whole(s, p, way):
        n = len(piece(s, p, way))
        a_sems, b_sems = ring_sems(s, p, way)
        return (
            copy(wa.at[0, 0:n], wa.at[0, 0:n], *a_sems, "sp_0", z),
            copy(wb.at[0, 0:n], wb.at[0, 0:n], *b_sems, "sp_1", y),
        )

    def send(s, p, only=None):
        for way in range(2):
            back, on = (down, up) if way == 0 else (up, down)
            a_sems, b_sems = ring_sems(s, p, way)
            n, m = back(z, s - 1), back(y, s - 1)
            for e in piece(s, p, way) if only is None else only:
                a, b = wa.at[n, up(y, e)], wb.at[up(z, e), m]
                copy(a, a, *a_sems, "sp_0", on(z, 1)).start()
                copy(b, b, *b_sems, "sp_1", on(y, 1)).start()
            if piece(s, p, way) and (only is None or only[-1] == PIECES[p][-1]):
                held.extend(whole(s, p, way))

    def take(s, p):
        for way in range(2):
            if piece(s, p, way):
                for c in whole(s, p, way):
                    c.wait_recv()

    def begin():
        pl.semaphore_wait(barrier, 21)
        first(1, True)
        send(1, 0, (0,))
        for j in (1, 3, 2):
            go(copy(pb.at[tp], pb.at[tp], p1s.at[j - 1], p1r.at[j - 1], "tp", 2 * up(xc, j, 4) + core))
        go(copy(pb.at[tp], pb.at[tp], p2s.at[0], p2r.at[0], "tp", partner))

    sides = []
    for d in range(2):
        if d == 1:
            begin()
        k, passed, written, g_all, vw, qc = local_mixer(
            q, key, val, inv, fade_ref[d].astype(F32), amend_ref[d].astype(F32),
            dot(extra_ref[d], spread_heads, 0, 0), d
        )
        passed, written = passed.astype(BF16), written.astype(BF16)
        for part in range(4):
            c1s[4 * d + part] = jnp.concatenate([passed, written[16 * part : 16 * part + 16]], 0)
        sides.append((k, g_all, vw, qc))
    for j in order:
        w = up(y, j)
        go(copy(c1s.at[w], c1r.at[y], x1s.at[j - 1], x1r.at[j - 1], "sp_1", w))
    c1r[y] = c1s[y]
    first(1, False)
    first(2, True)
    send(1, 0, (1, 7))

    for c in late_copies:
        c.wait()
    reads = []
    for k, g_all, vw, qc in sides:
        oy = bdot(g_all, vw)
        reads.append((oy[:, :128], (qc - oy[:, 128:]).astype(BF16)))
    bonus = dot(q * (sides[0][0] + sides[1][0]) * bonus_ref[...], ones) * val

    first(2, False)
    first(3, True)
    send(1, 1)

    for j in order:
        copy(c1s.at[y], c1r.at[down(y, j)], x1s.at[j - 1], x1r.at[j - 1], "sp_1", y).wait_recv()
    side = y // 4
    both = jnp.where(iota((64, 128), 0) == (iota((64, 128), 1) & 63), 1.0, 0.0).astype(F32)
    joined = jnp.concatenate([both, jnp.zeros((16, 128), F32)], 0)
    fresh = jnp.zeros((64, 128), F32)
    prefixes = []
    for n in range(8):
        prefixes.append(joined)
        block = c1r[n + side * (7 - 2 * n)]
        joined = bdot(joined, expand(block[:64])) + jnp.concatenate(
            [fresh, block[64:].astype(F32)], 0
        )
    c2s[...] = joined.astype(BF16)
    c2r[z] = joined.astype(BF16)
    for j in order:
        go(copy(c2s, c2r.at[z], x2s.at[j - 1], x2r.at[j - 1], "sp_0", up(z, j)))

    first(3, False)
    first(4, True)
    send(1, 2, (3, 5))
    take(1, 0)
    send(2, 0)
    first(4, False)
    send(1, 2, (4,))
    take(1, 1)
    send(2, 1)

    for j in order:
        copy(c2s, c2r.at[down(z, j)], x2s.at[j - 1], x2r.at[j - 1], "sp_0", z).wait_recv()
    entering = jnp.zeros((16, 128), F32)
    for n in range(8):
        at = n + side * (7 - 2 * n)
        block = c2r[at]
        new = bdot(entering, expand(block[:64])) + block[64:].astype(F32)
        before = (1 - 2 * side) * (z - at) > 0
        entering = jnp.where(before, new, entering)
    for n in range(8):
        before = prefixes[n]
        c3s[n + side * (7 - 2 * n)] = (
            bdot(entering, expand(before[:64])) + before[64:]
        ).astype(BF16)
    for j in order:
        w = up(y, j)
        go(copy(c3s.at[w], c3r.at[y], x3s.at[j - 1], x3r.at[j - 1], "sp_1", w))
    c3r[y] = c3s[y]

    take(1, 2)
    send(2, 2)
    take(2, 0)
    send(3, 0)

    for j in (1, 3, 2):
        at = 2 * down(xc, j, 4) + core
        copy(pb.at[tp], pb.at[at], p1s.at[j - 1], p1r.at[j - 1], "tp", tp).wait_recv()
        go(copy(pb.at[at], pb.at[at], p3s.at[j - 1], p3r.at[j - 1], "tp", partner))

    take(2, 1)
    send(3, 1)

    for j in order:
        copy(c3s.at[y], c3r.at[down(y, j)], x3s.at[j - 1], x3r.at[j - 1], "sp_1", y).wait_recv()
    summed = jnp.zeros((64, 128), F32)
    for d in range(2):
        state = jnp.concatenate([c3r[4 * d + part] for part in range(4)], 0)
        summed = summed + reads[d][0] + bdot(reads[d][1], expand(state), 1, 1)
    center = dot(summed, ones) * (1.0 / 64)
    away = summed - center
    spread = dot(away * away, ones) * (1.0 / 64)
    normed = away * lax.rsqrt(spread + GROUP_EPS) * again_ref[...]
    mixed = (normed + bonus) * valve_ref[...].astype(F32)
    mb[tp] = mixed.astype(BF16)
    for j in order:
        go(copy(mb.at[tp], mb.at[tp], ms.at[j - 1], mr.at[j - 1], "tp", up(tp, j)))
    take(2, 2)
    send(3, 2)
    copy(pb.at[tp], pb.at[partner], p2s.at[0], p2r.at[0], "tp", tp).wait_recv()
    for j in (1, 3, 2):
        at = 2 * down(xc, j, 4) + 1 - core
        copy(pb.at[at], pb.at[at], p3s.at[j - 1], p3r.at[j - 1], "tp", tp).wait_recv()
    for j in order:
        copy(mb.at[tp], mb.at[down(tp, j)], ms.at[j - 1], mr.at[j - 1], "tp", tp).wait_recv()

    rows = jnp.concatenate([mb[n] for n in range(8)], 1)

    def project(n, carry):
        cols = pl.ds(pl.multiple_of(n * 256, 256), 256)
        weights = pb[:, :, cols].reshape(1024, 256)
        midf[:, cols] = RESIDUAL_SCALE * skip_ref[:, cols].astype(F32) + bdot(rows, weights)
        return carry

    lax.fori_loop(0, 8, project, 0)

    def layer_norm(x, gain):
        center = jnp.mean(x, -1, keepdims=True)
        away = x - center
        spread = jnp.mean(away * away, -1, keepdims=True)
        return away * lax.rsqrt(spread + NORM_EPS) * gain

    for n in range(8):
        part = slice(8 * n, 8 * n + 8)
        normal = layer_norm(midf[part, :], mgain_ref[...]).astype(BF16)
        midf[part, :] = normal.astype(F32)
    midb[...] = midf[...].astype(BF16)

    take(3, 0)
    send(4, 0)
    take(3, 1)
    send(4, 1)
    take(3, 2)
    send(4, 2)

    gu[...] = jnp.zeros_like(gu)

    def widen(n):
        mid = midb[:, pl.ds(pl.multiple_of(n * 256, 256), 256)]
        gu[:, :1152] += bdot(mid, wa[n].reshape(256, 1152))

    def widen_near(n, carry):
        widen(up(z, n + 5))
        return carry

    def widen_rest(n, carry):
        mid = midb[:, pl.ds(pl.multiple_of(n * 256, 256), 256)]
        gu[:, 1152:] += bdot(mid, wb[n, :, :, :256].reshape(256, 256))
        return carry

    lax.fori_loop(0, 7, widen_near, 0)
    take(4, 0)
    take(4, 1)
    take(4, 2)
    widen(up(z, 4))
    lax.fori_loop(0, 8, widen_rest, 0)

    gate, wide = gu[:, :640], gu[:, 640:1280]
    tail = gu[:, 1280:]
    main = gate / (1.0 + jnp.exp(-gate)) * wide
    rest = tail / (1.0 + jnp.exp(-tail)) * pltpu.roll(tail, 64, 1)
    rest = jnp.where(iota((64, 128), 1) < 64, rest, 0.0)
    inner = jnp.concatenate([main, rest], 1).astype(BF16)

    def shrink(n, carry):
        cols = pl.ds(pl.multiple_of(n * 256, 256), 256)
        share = bdot(inner, wb[n, :, :, 256:].reshape(256, 768), 1, 1)
        for m in range(8):
            rs[m, :, cols] = share[8 * m : 8 * m + 8].astype(BF16)
        return carry

    def share_copy(half, j, source, target):
        cols = slice(1024 * half, 1024 * half + 1024)
        return copy(
            rs.at[target, :, cols], rr.at[source, :, cols], ds.at[half, j - 1], dr.at[half, j - 1], "tp", target
        )

    for half in range(2):
        lax.fori_loop(4 * half, 4 * half + 4, shrink, 0)
        for j in order:
            go(share_copy(half, j, tp, up(tp, j)))
    rr[tp] = rs[tp]
    for half in range(2):
        for j in order:
            share_copy(half, j, down(tp, j), tp).wait_recv()
    total = RESIDUAL_SCALE * midf[pl.ds(pl.multiple_of(tp * 8, 8), 8), :]
    for n in range(8):
        total = total + rr[n].astype(F32)
    out_ref[...] = layer_norm(total, cgain_ref[...]).astype(BF16)
    for c in sent + held:
        c.wait_send()


def shards(
    skip, reading, labels, payloads, valve, fading, amend, extra, bonus, again, projector,
    mgain, gate, wide, shrink, cgain,
):
    down_rows = jnp.swapaxes(shrink, 0, 1)
    dma = pltpu.SemaphoreType.DMA
    sems = [(2, 4)] * 4 + [(2, 4, 3)] * 4 + [(3,), (3,), (1,), (1,), (3,), (3,)] + [(7,)] * 8 + [(2, 7)] * 2 + [(6,), (4,), (6,)]
    return pl.pallas_call(
        body,
        out_shape=jax.ShapeDtypeStruct((8, 2048), BF16),
        in_specs=[pl.BlockSpec(memory_space=pltpu.HBM)] * 16,
        out_specs=pl.BlockSpec(memory_space=pltpu.VMEM),
        scratch_shapes=[
            pltpu.VMEM((64, 2048), BF16),
            pltpu.VMEM((64, 128), BF16),
            pltpu.VMEM((64, 128), BF16),
            pltpu.VMEM((64, 128), BF16),
            pltpu.VMEM((64, 128), BF16),
            pltpu.VMEM((2, 64, 128), BF16),
            pltpu.VMEM((2, 64, 128), BF16),
            pltpu.VMEM((2, 2, 64), F32),
            pltpu.VMEM((1, 128), F32),
            pltpu.VMEM((1, 128), F32),
            pltpu.VMEM((1, 2048), F32),
            pltpu.VMEM((32, 704), BF16),
            pltpu.VMEM((32, 704), BF16),
            pltpu.VMEM((32, 704), BF16),
            pltpu.VMEM((1, 2048), F32),
            pltpu.VMEM((8, 8, 32, WA_COLS), BF16),
            pltpu.VMEM((8, 8, 32, WB_COLS), BF16),
            pltpu.VMEM((8, 128, 2048), BF16),
            pltpu.VMEM((8, 80, 128), BF16),
            pltpu.VMEM((8, 80, 128), BF16),
            pltpu.VMEM((80, 128), BF16),
            pltpu.VMEM((8, 80, 128), BF16),
            pltpu.VMEM((8, 16, 128), BF16),
            pltpu.VMEM((8, 16, 128), BF16),
            pltpu.VMEM((8, 64, 128), BF16),
            pltpu.VMEM((8, 8, 2048), BF16),
            pltpu.VMEM((8, 8, 2048), BF16),
            pltpu.VMEM((64, 2048), F32),
            pltpu.VMEM((64, 2048), BF16),
            pltpu.VMEM((64, 1408), F32),
        ]
        + [dma(s) for s in sems],
        compiler_params=pltpu.CompilerParams(
            collective_id=0, has_side_effects=True, vmem_limit_bytes=67043328
        ),
    )(
        skip, reading, labels, payloads, valve, fading, amend, extra, bonus.reshape(1, 128),
        again.reshape(1, 128), projector, mgain.reshape(1, 2048), gate, wide,
        down_rows, cgain.reshape(1, 2048),
    )


def solution(mesh):
    finer = Mesh(mesh.devices.reshape(8, 8, mesh.shape["tp"]), ("sp_0", "sp_1", "tp"))
    placed = (
        P(SP, None),
        P(SP, "tp"),
        P(SP, "tp"),
        P(SP, "tp"),
        P(SP, "tp"),
        P(None, SP, "tp"),
        P(None, SP, "tp"),
        P(None, "tp", SP),
        P("tp"),
        P("tp"),
        P("tp", None),
        P(),
        P(SP, "tp"),
        P(SP, "tp"),
        P("tp", SP),
        P(),
    )
    return jax.shard_map(
        shards, mesh=finer, in_specs=placed, out_specs=P(SP_TP, None), check_vma=False
    )
```

```python
import jax
import jax.numpy as jnp
from jax import lax
from jax.experimental import pallas as pl
from jax.experimental.pallas import tpu as pltpu
from jax.sharding import Mesh
from jax.sharding import PartitionSpec as P

SP = ("sp_0", "sp_1")
SP_TP = ("sp_0", "sp_1", "tp")
MESH = pl.DeviceIdType.MESH
F32 = jnp.float32
BF16 = jnp.bfloat16
HIGHEST = lax.Precision.HIGHEST

RESIDUAL_SCALE = 2.0**0.25
NORM_EPS = 1e-05
GROUP_EPS = 0.00064
KEY_EPS = 1e-06
HALF_EXP = 0.6065306597126334

TOK = 64
LANES = 128
WA_COLS = 1152
WB_COLS = 1024
PIECES = ((0, 1, 7), (2, 6), (3, 5, 4))


def dot(a, b, ca=1, cb=0):
    return lax.dot_general(
        a, b, (((ca,), (cb,)), ((), ())), precision=HIGHEST, preferred_element_type=F32
    )


def bdot(a, b, ca=1, cb=0):
    return lax.dot_general(
        a.astype(BF16), b.astype(BF16), (((ca,), (cb,)), ((), ())), preferred_element_type=F32
    )


def iota(shape, dim):
    return lax.broadcasted_iota(jnp.int32, shape, dim)


def expand(x):
    lane = iota(x.shape, 1)
    zero = jnp.zeros_like(x)
    return jnp.concatenate([jnp.where(lane < 64, x, zero), jnp.where(lane >= 64, x, zero)], 0)


def fold(z):
    half = z.shape[0] // 2
    return z[:half] + z[half:]


def head_ones():
    return jnp.where((iota((128, 128), 0) < 64) == (iota((128, 128), 1) < 64), 1.0, 0.0).astype(F32)


def local_mixer(q, key, val, inv, fade, amend, extra, d):
    row, col = iota((64, 64), 0), iota((64, 64), 1)
    k = key * jax.nn.sigmoid(amend)
    logw = extra - jax.nn.sigmoid(fade) * HALF_EXP
    tri = jnp.where(col <= row if d == 0 else col >= row, 1.0, 0.0).astype(F32)
    c = dot(tri, logw)
    cx = c - logw
    end = c[63:64] if d == 0 else c[0:1]
    un = key * inv * inv
    erase_rows, read_rows = [], []
    for i in range(4):
        lo = 16 * i
        ref = cx[lo : lo + 1] if d == 0 else cx[lo + 15 : lo + 16]
        kk = k * jnp.exp(jnp.minimum(ref - c, 60.0))
        lu = un[lo : lo + 16] * jnp.exp(cx[lo : lo + 16] - ref)
        lq = q[lo : lo + 16] * jnp.exp(c[lo : lo + 16] - ref)
        res = bdot(jnp.concatenate([lu, lq], 0), expand(kk), 1, 1)
        erase_rows.append(res[:16])
        read_rows.append(res[16:])
    m_all = jnp.concatenate(erase_rows, 0)
    g_all = jnp.concatenate(read_rows, 0)
    rt, ct = iota((64, 128), 0), iota((64, 128), 1) & 63
    m_all = expand(jnp.where(ct < rt if d == 0 else ct > rt, m_all, 0.0))
    g_all = jnp.where(ct <= rt if d == 0 else ct >= rt, g_all, 0.0)
    r, cc = iota((128, 128), 0), iota((128, 128), 1)
    eye = jnp.where(r == cc, 1.0, 0.0).astype(F32)
    inverse = eye - jnp.where((r >> 1) == (cc >> 1), m_all, 0.0)
    for b in range(1, 6):
        off = jnp.where(((r >> (b + 1)) == (cc >> (b + 1))) & ((r >> b) != (cc >> b)), m_all, 0.0)
        inverse = inverse - dot(dot(inverse, off), inverse)
    ut = un * jnp.exp(cx)
    vw = dot(inverse, jnp.concatenate([expand(val), expand(ut)], 1))
    kend = expand(k * jnp.exp(end - c))
    z = bdot(vw, kend, 0, 0)
    written = fold(z[:128])
    passed = jnp.where(rt == ct, jnp.exp(end), 0.0) - fold(z[128:])
    return k, passed, written, g_all, vw, q * jnp.exp(c)


def body(
    skip_hbm, q_hbm, key_hbm, val_hbm, valve_hbm, fade_hbm, amend_hbm, extra_hbm, bonus_hbm,
    again_hbm, proj_hbm, mgain_hbm, gate_hbm, wide_hbm, drow_hbm, cgain_hbm, out_ref,
    skip_ref, q_ref, key_ref, val_ref, valve_ref, fade_ref, amend_ref, extra_ref, bonus_ref,
    again_ref, mgain_ref, gate_ref, wide_ref, drow_ref, cgain_ref,
    wa, wb, pb, c1s, c1r, c2s, c2r, c3s, c3r, mb, rs, rr, midf, midb, gu,
    a1s, a1r, b1s, b1r, a2s, a2r, b2s, b2r, p1s, p1r, p2s, p2r, p3s, p3r,
    x1s, x1r, x2s, x2r, x3s, x3r, ms, mr, ds, dr, early, weighty, late, relay,
):
    z, y, tp = lax.axis_index("sp_0"), lax.axis_index("sp_1"), lax.axis_index("tp")
    xc, core = tp // 2, tp % 2
    partner = tp + 1 - 2 * core

    def up(at, j, n=8):
        return lax.rem(at + j, n)

    def down(at, j, n=8):
        return lax.rem(at + n - j, n)

    def copy(src, dst, send, recv, axis, at):
        return pltpu.make_async_remote_copy(
            src_ref=src, dst_ref=dst, send_sem=send, recv_sem=recv,
            device_id={axis: at}, device_id_type=MESH,
        )

    barrier = pltpu.get_barrier_semaphore()
    near = [("sp_0", up(z, 1)), ("sp_0", down(z, 1)), ("sp_1", up(y, 1)), ("sp_1", down(y, 1))]
    for axis, at in near + [("tp", up(tp, j)) for j in range(1, 8)]:
        pl.semaphore_signal(barrier, inc=1, device_id={axis: at}, device_id_type=MESH)

    def pass_word(n):
        if n > 0:
            pl.semaphore_wait(relay.at[n - 1], 4)
        if n < 3:
            for axis, at in near:
                pl.semaphore_signal(relay.at[n], inc=1, device_id={axis: at}, device_id_type=MESH)


    def fetch(pairs, sem):
        copies = [pltpu.make_async_copy(a, b, sem.at[n]) for n, (a, b) in enumerate(pairs)]
        for c in copies:
            c.start()
        return copies

    early_copies = fetch(
        (
            (key_hbm, key_ref), (fade_hbm, fade_ref), (amend_hbm, amend_ref), (extra_hbm, extra_ref),
            (q_hbm, q_ref), (val_hbm, val_ref),
        ),
        early,
    )
    weight_copies = fetch(
        ((gate_hbm, gate_ref), (wide_hbm, wide_ref), (drow_hbm, drow_ref), (proj_hbm, pb.at[tp])), weighty
    )
    late_copies = fetch(
        (
            (valve_hbm, valve_ref), (bonus_hbm, bonus_ref), (again_hbm, again_ref),
            (skip_hbm, skip_ref), (mgain_hbm, mgain_ref), (cgain_hbm, cgain_ref),
        ),
        late,
    )
    sent = []
    order = (1, 7, 2, 6, 3, 5, 4)

    def go(c):
        c.start()
        sent.append(c)

    for c in weight_copies:
        c.wait()
    wa[z, y, :, :384] = gate_ref[:, :384]
    wa[z, y, :, 384:768] = wide_ref[:, :384]
    wa[z, y, :, 768:] = drow_ref[:, :384]
    wb[z, y, :, :256] = gate_ref[:, 384:640]
    wb[z, y, :, 256:512] = wide_ref[:, 384:640]
    wb[z, y, :, 512:640] = jnp.concatenate([gate_ref[:, 640:], wide_ref[:, 640:]], 1)
    wb[z, y, :, 640:896] = drow_ref[:, 384:640]
    wb[z, y, :, 896:] = jnp.concatenate([drow_ref[:, 640:], jnp.zeros((32, 64), BF16)], 1)
    def first(k, start):
        for way in range(2):
            back, on = (down, up) if way == 0 else (up, down)
            part = slice(0, 32) if k < 4 else slice(16 * way, 16 * way + 16)
            at = k - 1 if start else k
            a, b = wa.at[z, back(y, at), part], wb.at[back(z, at), y, part]
            a = copy(a, a, a1s.at[way, k - 1], a1r.at[way, k - 1], "sp_1", on(y, 1))
            b = copy(b, b, b1s.at[way, k - 1], b1r.at[way, k - 1], "sp_0", on(z, 1))
            if start:
                go(a)
                go(b)
            else:
                a.wait_recv()
                b.wait_recv()

    held = []

    def piece(s, p, way):
        every, ahead, after = (0, WA_COLS, 0, WB_COLS), (0, 768, 0, 640), (768, WA_COLS, 640, WB_COLS)
        if s < 4:
            return PIECES[p], every
        if way == 0:
            return (((0, 1, 7), ahead), ((2,), ahead), ((0, 1, 7, 2), after))[p]
        return (((6, 3, 5, 4), after), ((6,), ahead), ((3, 5, 4), ahead))[p]

    def ring_sems(s, p, way):
        return (a2s.at[way, s - 1, p], a2r.at[way, s - 1, p]), (b2s.at[way, s - 1, p], b2r.at[way, s - 1, p])

    def whole(s, p, way):
        blocks, (a0, a1, b0, b1) = piece(s, p, way)
        a_sems, b_sems = ring_sems(s, p, way)
        a, b = wa.at[0, 0 : len(blocks), :, a0:a1], wb.at[0, 0 : len(blocks), :, b0:b1]
        return copy(a, a, *a_sems, "sp_0", z), copy(b, b, *b_sems, "sp_1", y)

    def send(s, p, only=None, ways=(0, 1)):
        for way in ways:
            back, on = (down, up) if way == 0 else (up, down)
            blocks, (a0, a1, b0, b1) = piece(s, p, way)
            a_sems, b_sems = ring_sems(s, p, way)
            n, m = back(z, s - 1), back(y, s - 1)
            for e in blocks if only is None else only:
                a, b = wa.at[n, up(y, e), :, a0:a1], wb.at[up(z, e), m, :, b0:b1]
                copy(a, a, *a_sems, "sp_0", on(z, 1)).start()
                copy(b, b, *b_sems, "sp_1", on(y, 1)).start()
            if only is None or only[-1] == blocks[-1]:
                held.extend(whole(s, p, way))

    def take(s, p, ways=(0, 1)):
        for way in ways:
            for c in whole(s, p, way):
                c.wait_recv()

    def begin():
        pl.semaphore_wait(barrier, 11)
        pass_word(0)
        first(1, True)
        send(1, 0, (0,))
        for j in (1, 3, 2):
            go(copy(pb.at[tp], pb.at[tp], p1s.at[j - 1], p1r.at[j - 1], "tp", 2 * up(xc, j, 4) + core))
        go(copy(pb.at[tp], pb.at[tp], p2s.at[0], p2r.at[0], "tp", partner))

    begin()
    for c in early_copies:
        c.wait()
    q, key, val = q_ref[...].astype(F32), key_ref[...].astype(F32), val_ref[...].astype(F32)
    ones = head_ones()
    spread_heads = jnp.where((iota((2, 128), 1) >> 6) == iota((2, 128), 0), 1.0, 0.0).astype(F32)
    inv = lax.rsqrt(dot(key * key, ones) + KEY_EPS)
    sides = []
    for d in range(2):
        pass_word(d + 1)
        if d == 1:
            first(1, False)
            first(2, True)
            send(1, 0, (1, 7))
        k, passed, written, g_all, vw, qc = local_mixer(
            q, key, val, inv, fade_ref[d].astype(F32), amend_ref[d].astype(F32),
            dot(extra_ref[d], spread_heads, 0, 0), d
        )
        passed, written = passed.astype(BF16), written.astype(BF16)
        for part in range(4):
            c1s[4 * d + part] = jnp.concatenate([passed, written[16 * part : 16 * part + 16]], 0)
        sides.append((k, g_all, vw, qc))
    pass_word(3)
    for j in order:
        w = up(y, j)
        go(copy(c1s.at[w], c1r.at[y], x1s.at[j - 1], x1r.at[j - 1], "sp_1", w))
    c1r[y] = c1s[y]

    for c in late_copies:
        c.wait()
    reads = []
    for k, g_all, vw, qc in sides:
        oy = bdot(g_all, vw)
        reads.append((oy[:, :128], (qc - oy[:, 128:]).astype(BF16)))
    bonus = dot(q * (sides[0][0] + sides[1][0]) * bonus_ref[...], ones) * val

    first(2, False)
    first(3, True)
    send(1, 1)

    for j in order:
        copy(c1s.at[y], c1r.at[down(y, j)], x1s.at[j - 1], x1r.at[j - 1], "sp_1", y).wait_recv()
    side = y // 4
    both = jnp.where(iota((64, 128), 0) == (iota((64, 128), 1) & 63), 1.0, 0.0).astype(F32)
    joined = jnp.concatenate([both, jnp.zeros((16, 128), F32)], 0)
    fresh = jnp.zeros((64, 128), F32)
    prefixes = []
    for n in range(8):
        prefixes.append(joined)
        block = c1r[n + side * (7 - 2 * n)]
        joined = bdot(joined, expand(block[:64])) + jnp.concatenate(
            [fresh, block[64:].astype(F32)], 0
        )
    c2s[...] = joined.astype(BF16)
    c2r[z] = joined.astype(BF16)
    for j in order:
        go(copy(c2s, c2r.at[z], x2s.at[j - 1], x2r.at[j - 1], "sp_0", up(z, j)))

    first(3, False)
    first(4, True)
    send(1, 2, (3, 5))
    take(1, 0)
    send(2, 0)
    first(4, False)
    send(1, 2, (4,))
    take(1, 1)
    send(2, 1)

    for j in order:
        copy(c2s, c2r.at[down(z, j)], x2s.at[j - 1], x2r.at[j - 1], "sp_0", z).wait_recv()
    entering = jnp.zeros((16, 128), F32)
    for n in range(8):
        at = n + side * (7 - 2 * n)
        block = c2r[at]
        new = bdot(entering, expand(block[:64])) + block[64:].astype(F32)
        before = (1 - 2 * side) * (z - at) > 0
        entering = jnp.where(before, new, entering)
    for n in range(8):
        before = prefixes[n]
        c3s[n + side * (7 - 2 * n)] = (
            bdot(entering, expand(before[:64])) + before[64:]
        ).astype(BF16)
    for j in order:
        w = up(y, j)
        go(copy(c3s.at[w], c3r.at[y], x3s.at[j - 1], x3r.at[j - 1], "sp_1", w))
    c3r[y] = c3s[y]

    take(1, 2)
    send(2, 2)
    take(2, 0)
    send(3, 0)

    for j in (1, 3, 2):
        at = 2 * down(xc, j, 4) + core
        copy(pb.at[tp], pb.at[at], p1s.at[j - 1], p1r.at[j - 1], "tp", tp).wait_recv()
        go(copy(pb.at[at], pb.at[at], p3s.at[j - 1], p3r.at[j - 1], "tp", partner))

    take(2, 1)
    send(3, 1)

    for j in order:
        copy(c3s.at[y], c3r.at[down(y, j)], x3s.at[j - 1], x3r.at[j - 1], "sp_1", y).wait_recv()
    summed = jnp.zeros((64, 128), F32)
    for d in range(2):
        state = jnp.concatenate([c3r[4 * d + part] for part in range(4)], 0)
        summed = summed + reads[d][0] + bdot(reads[d][1], expand(state), 1, 1)
    center = dot(summed, ones) * (1.0 / 64)
    away = summed - center
    spread = dot(away * away, ones) * (1.0 / 64)
    normed = away * lax.rsqrt(spread + GROUP_EPS) * again_ref[...]
    mixed = (normed + bonus) * valve_ref[...].astype(F32)
    mb[tp] = mixed.astype(BF16)
    for j in order:
        go(copy(mb.at[tp], mb.at[tp], ms.at[j - 1], mr.at[j - 1], "tp", up(tp, j)))
    take(2, 2)
    send(3, 2)
    copy(pb.at[tp], pb.at[partner], p2s.at[0], p2r.at[0], "tp", tp).wait_recv()
    for j in (1, 3, 2):
        at = 2 * down(xc, j, 4) + 1 - core
        copy(pb.at[at], pb.at[at], p3s.at[j - 1], p3r.at[j - 1], "tp", tp).wait_recv()
    for j in order:
        copy(mb.at[tp], mb.at[down(tp, j)], ms.at[j - 1], mr.at[j - 1], "tp", tp).wait_recv()

    rows = jnp.concatenate([mb[n] for n in range(8)], 1)

    def project(n, carry):
        cols = pl.ds(pl.multiple_of(n * 256, 256), 256)
        weights = pb[:, :, cols].reshape(1024, 256)
        midf[:, cols] = RESIDUAL_SCALE * skip_ref[:, cols].astype(F32) + bdot(rows, weights)
        return carry

    lax.fori_loop(0, 8, project, 0)

    def layer_norm(x, gain):
        center = jnp.mean(x, -1, keepdims=True)
        away = x - center
        spread = jnp.mean(away * away, -1, keepdims=True)
        return away * lax.rsqrt(spread + NORM_EPS) * gain

    for n in range(8):
        part = slice(8 * n, 8 * n + 8)
        normal = layer_norm(midf[part, :], mgain_ref[...]).astype(BF16)
        midf[part, :] = normal.astype(F32)
    midb[...] = midf[...].astype(BF16)

    take(3, 0)
    send(4, 0, None, (0,))
    take(3, 1)
    send(4, 1)
    send(4, 2, None, (0,))
    take(3, 2)
    send(4, 2, None, (1,))
    send(4, 0, None, (1,))

    gu[...] = jnp.zeros_like(gu)

    def widen(n):
        mid = midb[:, pl.ds(pl.multiple_of(n * 256, 256), 256)]
        gu[:, :768] += bdot(mid, wa[n, :, :, :768].reshape(256, 768))

    def widen_near(n, carry):
        widen(up(z, n + 5))
        return carry

    def widen_rest(n, carry):
        mid = midb[:, pl.ds(pl.multiple_of(n * 256, 256), 256)]
        gu[:, 768:] += bdot(mid, wb[n, :, :, :640].reshape(256, 640))
        return carry

    lax.fori_loop(0, 7, widen_near, 0)
    take(4, 0, (0,))
    take(4, 1)
    take(4, 2, (1,))
    widen(up(z, 4))
    lax.fori_loop(0, 8, widen_rest, 0)

    gate, wide = gu[:, :384], gu[:, 384:768]
    gate_b, wide_b, tail = gu[:, 768:1024], gu[:, 1024:1280], gu[:, 1280:]
    main = gate / (1.0 + jnp.exp(-gate)) * wide
    main_b = gate_b / (1.0 + jnp.exp(-gate_b)) * wide_b
    rest = tail / (1.0 + jnp.exp(-tail)) * pltpu.roll(tail, 64, 1)
    rest = jnp.where(iota((64, 128), 1) < 64, rest, 0.0)
    inner = main.astype(BF16)
    inner_b = jnp.concatenate([main_b, rest], 1).astype(BF16)
    take(4, 2, (0,))
    take(4, 0, (1,))

    def shrink(n, carry):
        cols = pl.ds(pl.multiple_of(n * 256, 256), 256)
        share = bdot(inner, wa[n, :, :, 768:].reshape(256, 384), 1, 1)
        share += bdot(inner_b, wb[n, :, :, 640:].reshape(256, 384), 1, 1)
        for m in range(8):
            rs[m, :, cols] = share[8 * m : 8 * m + 8].astype(BF16)
        return carry

    def share_copy(half, j, source, target):
        cols = slice(512 * half, 512 * half + 512)
        return copy(
            rs.at[target, :, cols], rr.at[source, :, cols], ds.at[half, j - 1], dr.at[half, j - 1], "tp", target
        )

    for half in range(4):
        lax.fori_loop(2 * half, 2 * half + 2, shrink, 0)
        for j in order:
            go(share_copy(half, j, tp, up(tp, j)))
    rr[tp] = rs[tp]
    for half in range(4):
        for j in order:
            share_copy(half, j, down(tp, j), tp).wait_recv()
    total = RESIDUAL_SCALE * midf[pl.ds(pl.multiple_of(tp * 8, 8), 8), :]
    for n in range(8):
        total = total + rr[n].astype(F32)
    out_ref[...] = layer_norm(total, cgain_ref[...]).astype(BF16)
    for c in sent + held:
        c.wait_send()


def shards(
    skip, reading, labels, payloads, valve, fading, amend, extra, bonus, again, projector,
    mgain, gate, wide, shrink, cgain,
):
    down_rows = jnp.swapaxes(shrink, 0, 1)
    dma = pltpu.SemaphoreType.DMA
    sems = [(2, 4)] * 4 + [(2, 4, 3)] * 4 + [(3,), (3,), (1,), (1,), (3,), (3,)] + [(7,)] * 8 + [(4, 7)] * 2 + [(6,), (4,), (6,)]
    return pl.pallas_call(
        body,
        out_shape=jax.ShapeDtypeStruct((8, 2048), BF16),
        in_specs=[pl.BlockSpec(memory_space=pltpu.HBM)] * 16,
        out_specs=pl.BlockSpec(memory_space=pltpu.VMEM),
        scratch_shapes=[
            pltpu.VMEM((64, 2048), BF16),
            pltpu.VMEM((64, 128), BF16),
            pltpu.VMEM((64, 128), BF16),
            pltpu.VMEM((64, 128), BF16),
            pltpu.VMEM((64, 128), BF16),
            pltpu.VMEM((2, 64, 128), BF16),
            pltpu.VMEM((2, 64, 128), BF16),
            pltpu.VMEM((2, 2, 64), F32),
            pltpu.VMEM((1, 128), F32),
            pltpu.VMEM((1, 128), F32),
            pltpu.VMEM((1, 2048), F32),
            pltpu.VMEM((32, 704), BF16),
            pltpu.VMEM((32, 704), BF16),
            pltpu.VMEM((32, 704), BF16),
            pltpu.VMEM((1, 2048), F32),
            pltpu.VMEM((8, 8, 32, WA_COLS), BF16),
            pltpu.VMEM((8, 8, 32, WB_COLS), BF16),
            pltpu.VMEM((8, 128, 2048), BF16),
            pltpu.VMEM((8, 80, 128), BF16),
            pltpu.VMEM((8, 80, 128), BF16),
            pltpu.VMEM((80, 128), BF16),
            pltpu.VMEM((8, 80, 128), BF16),
            pltpu.VMEM((8, 16, 128), BF16),
            pltpu.VMEM((8, 16, 128), BF16),
            pltpu.VMEM((8, 64, 128), BF16),
            pltpu.VMEM((8, 8, 2048), BF16),
            pltpu.VMEM((8, 8, 2048), BF16),
            pltpu.VMEM((64, 2048), F32),
            pltpu.VMEM((64, 2048), BF16),
            pltpu.VMEM((64, 1408), F32),
        ]
        + [dma(s) for s in sems]
        + [pltpu.SemaphoreType.REGULAR((3,))],
        compiler_params=pltpu.CompilerParams(
            collective_id=0, has_side_effects=True, vmem_limit_bytes=67043328
        ),
    )(
        skip, reading, labels, payloads, valve, fading, amend, extra, bonus.reshape(1, 128),
        again.reshape(1, 128), projector, mgain.reshape(1, 2048), gate, wide,
        down_rows, cgain.reshape(1, 2048),
    )


def solution(mesh):
    finer = Mesh(mesh.devices.reshape(8, 8, mesh.shape["tp"]), ("sp_0", "sp_1", "tp"))
    placed = (
        P(SP, None),
        P(SP, "tp"),
        P(SP, "tp"),
        P(SP, "tp"),
        P(SP, "tp"),
        P(None, SP, "tp"),
        P(None, SP, "tp"),
        P(None, "tp", SP),
        P("tp"),
        P("tp"),
        P("tp", None),
        P(),
        P(SP, "tp"),
        P(SP, "tp"),
        P("tp", SP),
        P(),
    )
    return jax.shard_map(
        shards, mesh=finer, in_specs=placed, out_specs=P(SP_TP, None), check_vma=False
    )
```
